256 devices in a mesh: grp: 2 (over y), sp: 32 (over z, core), tp: 4 (over x).
Axes of the slice: x: 4, y: 2, z: 16, core: 2. Of those that a mesh axis runs over, the one named last changes fastest.
The devices are a block of a 4x16x16 slice.
Arguments:
- skip_stream: bfloat16 [8192, 2048], P(('grp', 'sp', 'tp')), parts along dimension 0, may hold values from -6 to 6
- wide_probe_logits: bfloat16 [8192, 512], P(('grp', 'sp'), 'tp'), parts along dimension 0, may hold values from -6 to 6
- narrow_probe_logits: bfloat16 [8192, 512], P(('grp', 'sp'), 'tp'), parts along dimension 0, may hold values from -6 to 6
- wide_decay_logits: bfloat16 [8192, 512], P(('grp', 'sp'), 'tp'), parts along dimension 0, may hold values from -7.5 to 7.5
- narrow_decay_logits: bfloat16 [8192, 512], P(('grp', 'sp'), 'tp'), parts along dimension 0, may hold values from -7.5 to 7.5
- wide_floor_complement: float32 [2, 512], P(None, 'tp'), may hold values from 3.4179688e-05 to 0.21
- narrow_floor_complement: float32 [2, 512], P(None, 'tp'), may hold values from 3.4179688e-05 to 0.21
- payloads: bfloat16 [8192, 1536], P(('grp', 'sp'), 'tp'), parts along dimension 0, may hold values from -6 to 6
- result_switch_logits: bfloat16 [8192, 1536], P(('grp', 'sp'), 'tp'), parts along dimension 0, may hold values from -6 to 6
- spike_decays: float32 [8192, 12], P(('grp', 'sp'), 'tp'), parts along dimension 0, may hold values from -1.5 to 0
- channel_scale_vector: float32 [1536], P('tp'), may hold values from 0.1 to 1.9
- result_mapping_matrix: bfloat16 [1536, 2048], P('tp'), may hold values from -0.15625 to 0.15625
- specialist_scale_vector: float32 [2048], replicated, may hold values from 0.1 to 1.9
- assignments: int32 [8192, 2], P(('grp', 'sp', 'tp')), parts along dimension 0, may hold values from 0 to 31, all different within a row; in each aligned block of 32 rows (0 to 31, 32 to 63, ...) at most 4 rows name the same one
- assignment_share: float32 [8192, 2], P(('grp', 'sp', 'tp')), parts along dimension 0, may hold values from 0.2 to 1
- specialist_switch_matrix: bfloat16 [32, 2048, 3584], P('sp', None, 'tp'), may hold values from -0.125 to 0.125
- specialist_raising_matrix: bfloat16 [32, 2048, 3584], P('sp', None, 'tp'), may hold values from -0.125 to 0.125
- specialist_lowering_matrix: bfloat16 [32, 3584, 2048], P('sp', 'tp'), may hold values from -0.09375 to 0.09375
Outputs:
- layer_output: bfloat16 [8192, 2048], P(('grp', 'sp', 'tp')), parts along dimension 0
The draws below stay inside these ranges and needn't reach their ends.
There are 2 independent parts, one for each index of `grp`. The reference program is written for one: setup_inputs(seed, part) draws one part's arguments, and reference() takes and returns one part's arrays. A program takes and returns all parts, laid end to end along the dimension named above; an argument that names none is the same for every part. Nothing has to cross between parts.
Inputs may be any that keep to these rules, and one draw needn't show every extreme that they name: `assignments`: each row names 2 different experts; in each aligned block of 32 rows no expert is named by more than 4 rows, a bound that some block reaches.
All inputs are finite; a program needn't handle non-finite values.
Results may differ from the reference program's by a relative error of at most 0.015.
Values may be sent and summed in bfloat16 or wider, within the bound.
No kernel may reach another device: no remote copies, remote signals or barrier semaphores. Data moves between devices by JAX's collectives and lax.ppermute only.
A program may use at most 128 MiB of HBM per device.

```python
import math
import jax
import jax.numpy as jnp
import numpy as np
from jax import lax

D = 2048
WIDE_GROUPS = 4
NARROW_GROUPS = 8
WIDE_LOOKUP_WIDTH = 128
NARROW_LOOKUP = 64
PAYLOAD_EXTENT = 128
DE = 3584
TOP = 2
BLOCK = 64
TOK_DEV = 128
ATTENTION_TALLY = 12
ELEMENT_TALLY = 4096
ROWS = 32
EXPERTS = 32
DE_PART = 896
CAP = 4
N_SP = 32
N_TP = 4


def gate_draw(key, column_count, salt):
    noise_part = jnp.clip(jax.random.normal(jax.random.fold_in(key, salt), (ELEMENT_TALLY, column_count), jnp.float32), -6.0, 6.0)
    shifts = jax.random.uniform(jax.random.fold_in(key, salt + 1), (ELEMENT_TALLY // TOK_DEV, 1), jnp.float32, -1.5, 1.5)
    return (noise_part + jnp.repeat(shifts, TOK_DEV, axis=0)).astype(jnp.bfloat16)


def leak_draw(key, channel_tally, lookup_extent, salt):
    slow_limit = 5
    slow_heads = jax.random.randint(jax.random.fold_in(key, salt), (2, channel_tally, 1), 0, 10) < slow_limit
    slow_rate = jnp.exp(jax.random.uniform(jax.random.fold_in(key, salt + 1), (2, channel_tally, 1), jnp.float32, math.log(0.2), 0.0)) / ELEMENT_TALLY
    fast_rate = jnp.exp(jax.random.uniform(jax.random.fold_in(key, salt + 2), (2, channel_tally, 1), jnp.float32, math.log(0.03), math.log(0.15)))
    channel_spread = jnp.exp(jax.random.uniform(jax.random.fold_in(key, salt + 3), (2, channel_tally, lookup_extent), jnp.float32, math.log(0.7), math.log(1.4)))
    return (jnp.where(slow_heads, slow_rate, fast_rate) * channel_spread).reshape(2, channel_tally * lookup_extent)


def draw_wide_decay_logits(key, part):
    return gate_draw(key, WIDE_GROUPS * WIDE_LOOKUP_WIDTH, 101)


def draw_narrow_decay_logits(key, part):
    return gate_draw(key, NARROW_GROUPS * NARROW_LOOKUP, 201)


def draw_wide_floor_complement(key, part):
    return leak_draw(key, WIDE_GROUPS, WIDE_LOOKUP_WIDTH, 301)


def draw_narrow_floor_complement(key, part):
    return leak_draw(key, NARROW_GROUPS, NARROW_LOOKUP, 401)


def draw_spike_decays(key, part):
    spike_locations = jax.random.randint(jax.random.fold_in(key, 501), (3, ATTENTION_TALLY), 0, ELEMENT_TALLY)
    memory_extent = jax.random.uniform(jax.random.fold_in(key, 502), (3, ATTENTION_TALLY), jnp.float32, -0.5, -0.22)
    locations = jnp.arange(ELEMENT_TALLY, dtype=jnp.int32)[:, None, None]
    return jnp.sum(jnp.where(locations == spike_locations[None], memory_extent[None], 0.0), axis=1).astype(jnp.float32)


def level_of(own_key, extent, cuts, low, high):
    factor_of, own = 1.0, jax.random.fold_in(own_key, 6)
    for dim, parts in cuts:
        steps = jnp.exp(jax.random.uniform(jax.random.fold_in(own, dim), (parts,), jnp.float32, low / len(cuts), high / len(cuts)))
        factor_of = factor_of * jnp.repeat(steps, extent[dim] // parts).reshape([-1 if axis == dim else 1 for axis in range(len(extent))])
    return factor_of


def routed_block(key, own, number, rows, count, top, most, skew):
    order = jax.random.permutation(key, count)
    crowded, ordinary = shares(count, rows * top, most, skew, True), shares(count, rows * top, most, skew, False)
    places = jnp.arange(count)

    def named(lengths, turn):
        used = int((lengths > 0).sum())
        fixed = max(1, used // 4)
        shifted = fixed + (places - fixed + turn * (used - fixed)) % max(1, count - fixed)
        return jnp.zeros((count,), jnp.int32).at[order[jnp.where(places < fixed, places, shifted)]].set(jnp.asarray(lengths, jnp.int32))

    lengths = jnp.where(number % 4 == 0, named(crowded, number // 4), named(ordinary, number - number // 4 - 1))
    mixed = jax.random.permutation(jax.random.fold_in(own, 3), count)
    giver, sink = mixed[0:count // 2 * 2:2], mixed[1:count // 2 * 2:2]
    slack = jnp.minimum(lengths[giver] - 1, most - lengths[sink]) // 2
    slack = jnp.where((giver == order[0]) | (sink == order[0]) | (lengths[sink] == 0), 0, jnp.maximum(slack, 0))
    shifted = jax.random.randint(jax.random.fold_in(own, 4), (count // 2,), 0, 1 << 20) % (slack + 1)
    lengths = lengths.at[giver].add(-shifted).at[sink].add(shifted)
    members = jnp.searchsorted(jnp.cumsum(lengths), jnp.arange(rows * top), side="right").astype(jnp.int32)
    grid = members.reshape(top, rows).T
    grid = grid[jax.random.permutation(jax.random.fold_in(own, 1), rows)]
    turn = jax.random.randint(jax.random.fold_in(own, 2), (rows, 1), 0, top)
    return jnp.take_along_axis(grid, (jnp.arange(top)[None, :] + turn) % top, axis=1)


def shares(number_of, total, limit, slope, full):
    loads = [(1 << 20) // math.isqrt(rank ** slope) + 1 for rank in range(1, number_of + 1)]
    largest = limit if full else min(limit, max(-(-total // number_of), total * loads[0] // sum(loads)))
    least = 1 if total - largest >= number_of - 1 else 0
    given, spare = [largest] + [least] * (number_of - 1), total - largest - least * (number_of - 1)
    while spare > 0:
        movable = [i for i in range(1, number_of) if given[i] < largest] or [i for i in range(1, number_of) if given[i] < limit]
        pool, remaining = sum([loads[i] for i in movable]), spare
        for i in movable:
            addition = min(limit - given[i], max(1, remaining * loads[i] // pool), spare)
            given[i] = given[i] + addition
            spare = spare - addition
    return np.array(given)


def gaussian(rng, dims, scale, limit, cuts=(), held_as=jnp.bfloat16):
    gain = level_of(rng, dims, cuts, -0.22, 0.18) if cuts else 1.0
    entries = jax.random.normal(rng, dims, jnp.float32) * scale * gain
    return jnp.minimum(jnp.maximum(entries, -limit), limit).astype(held_as)


def setup_inputs(seed: int = 0, part: int = 0) -> dict:
    keys = jax.random.split(jax.random.key(seed), 19)
    part_splits = jax.random.split(jax.random.fold_in(keys[18], part), 19)
    skip_stream = gaussian(part_splits[0], (ELEMENT_TALLY, D), 1.0, 6.0, ((0, 128),))
    wide_probe_logits = gaussian(part_splits[1], (ELEMENT_TALLY, WIDE_GROUPS * WIDE_LOOKUP_WIDTH), 1.0, 6.0, ((0, 32), (1, 4)))
    narrow_probe_logits = gaussian(part_splits[2], (ELEMENT_TALLY, NARROW_GROUPS * NARROW_LOOKUP), 1.0, 6.0, ((0, 32), (1, 4)))
    wide_decay_logits = draw_wide_decay_logits(jax.random.fold_in(jax.random.fold_in(keys[18], part), 71), part)
    narrow_decay_logits = draw_narrow_decay_logits(jax.random.fold_in(jax.random.fold_in(keys[18], part), 71), part)
    wide_floor_complement = draw_wide_floor_complement(jax.random.fold_in(keys[18], 71), part)
    narrow_floor_complement = draw_narrow_floor_complement(jax.random.fold_in(keys[18], 71), part)
    payloads = gaussian(part_splits[7], (ELEMENT_TALLY, ATTENTION_TALLY * PAYLOAD_EXTENT), 1.0, 6.0, ((0, 32), (1, 4)))
    result_switch_logits = gaussian(part_splits[8], (ELEMENT_TALLY, ATTENTION_TALLY * PAYLOAD_EXTENT), 1.0, 6.0, ((0, 32), (1, 4)))
    spike_decays = draw_spike_decays(jax.random.fold_in(jax.random.fold_in(keys[18], part), 71), part)
    channel_scale_vector = jnp.clip(1.0 + 0.18 * jax.random.normal(keys[10], (ATTENTION_TALLY * PAYLOAD_EXTENT,), jnp.float32), 0.1, 1.9)
    result_mapping_matrix = gaussian(keys[11], (ATTENTION_TALLY * PAYLOAD_EXTENT, D), (ATTENTION_TALLY * PAYLOAD_EXTENT) ** -0.5, 0.15625, ((0, 4),))
    specialist_scale_vector = jnp.clip(1.0 + 0.18 * jax.random.normal(keys[12], (D,), jnp.float32), 0.1, 1.9)
    assignments_keys = jax.random.split(jax.random.fold_in(part_splits[13], 1), ELEMENT_TALLY // ROWS)
    assignments_turns = jax.random.permutation(jax.random.fold_in(part_splits[13], 3), ELEMENT_TALLY // ROWS)
    assignments = jax.vmap(lambda own, number: routed_block(jax.random.fold_in(part_splits[13], 2), own, number, ROWS, EXPERTS, TOP, CAP, 2))(assignments_keys, assignments_turns).reshape((ELEMENT_TALLY, TOP))
    assignment_share = jnp.clip(0.2 + 0.8 * jax.random.uniform(part_splits[14], (ELEMENT_TALLY, TOP), jnp.float32) ** level_of(part_splits[14], (ELEMENT_TALLY, TOP), ((0, 128),), -0.2, 0.2), 0.2, 1.0)
    specialist_switch_matrix = gaussian(keys[15], (EXPERTS, D, DE), D ** -0.5, 0.125, ((0, 32), (2, 4)))
    specialist_raising_matrix = gaussian(keys[16], (EXPERTS, D, DE), D ** -0.5, 0.125, ((0, 32), (2, 4)))
    specialist_lowering_matrix = gaussian(keys[17], (EXPERTS, DE, D), DE ** -0.5, 0.09375, ((0, 32), (1, 4)))
    return dict(skip_stream=skip_stream, wide_probe_logits=wide_probe_logits, narrow_probe_logits=narrow_probe_logits, wide_decay_logits=wide_decay_logits, narrow_decay_logits=narrow_decay_logits, wide_floor_complement=wide_floor_complement, narrow_floor_complement=narrow_floor_complement, payloads=payloads, result_switch_logits=result_switch_logits, spike_decays=spike_decays, channel_scale_vector=channel_scale_vector, result_mapping_matrix=result_mapping_matrix, specialist_scale_vector=specialist_scale_vector, assignments=assignments, assignment_share=assignment_share, specialist_switch_matrix=specialist_switch_matrix, specialist_raising_matrix=specialist_raising_matrix, specialist_lowering_matrix=specialist_lowering_matrix)


epsilon = 1e-06

def switch_cumulants(decay_factor, floor_complement, spike_log_decay):
    initial_memory = jax.nn.sigmoid(-decay_factor)
    key_input = floor_complement * initial_memory
    keep_log_decay = jnp.log1p(-floor_complement * initial_memory) + spike_log_decay[:, :, None]
    return (key_input, keep_log_decay)

def block_pass(queries, key_input, memory_matrix, keep_log_decay, initial):
    series_extent = queries.shape[0]
    channel_tally = queries.shape[1]
    block_count = series_extent // BLOCK

    def to_blocks(tensor):
        return tensor.reshape(block_count, BLOCK, channel_tally, tensor.shape[-1]).transpose(0, 2, 1, 3)
    below_mask = jnp.tril(jnp.ones((BLOCK, BLOCK), dtype=bool))[None, :, :, None]

    def advance(carried, segment):
        query_block, key_block, value_block, decay_block = segment
        running = jnp.cumsum(decay_block, axis=1)
        log_gap = running[:, :, None, :] - running[:, None, :, :]
        weight = jnp.where(below_mask, jnp.exp(jnp.where(below_mask, log_gap, 0.0)), 0.0)
        scores = jnp.einsum('htd,hsd,htsd->hts', query_block, key_block, weight, precision=lax.Precision.HIGHEST)
        output = jnp.einsum('hts,hse->hte', scores, value_block, precision=lax.Precision.HIGHEST)
        output = output + jnp.einsum('htd,hde->hte', query_block * jnp.exp(running), carried, precision=lax.Precision.HIGHEST)
        closing = running[:, -1:, :]
        fresh = jnp.einsum('hsd,hse->hde', key_block * jnp.exp(closing - running), value_block, precision=lax.Precision.HIGHEST)
        carried = jnp.exp(closing[:, 0, :, None]) * carried + fresh
        return (carried, output)
    closing_state, outputs = lax.scan(advance, initial, (to_blocks(queries), to_blocks(key_input), to_blocks(memory_matrix), to_blocks(keep_log_decay)))
    return (outputs.transpose(0, 2, 1, 3).reshape(series_extent, channel_tally, -1), closing_state)

def twin_orientations(probe_logits, decay_factor, floor_complement, spike_log_decay, memory_matrix, lookup_extent):
    series_extent = probe_logits.shape[0]
    channel_tally = spike_log_decay.shape[1]
    queries = jax.nn.silu(probe_logits.astype(jnp.float32).reshape(series_extent, channel_tally, lookup_extent)) * lookup_extent ** (-0.5)
    decay_switch_level = decay_factor.astype(jnp.float32).reshape(series_extent, channel_tally, lookup_extent)
    initial = jnp.zeros((channel_tally, lookup_extent, memory_matrix.shape[-1]), jnp.float32)
    onward_lookup, onward_log_decay = switch_cumulants(decay_switch_level, floor_complement[0].reshape(channel_tally, lookup_extent), spike_log_decay)
    reverse_lookup, reverse_log_decay = switch_cumulants(decay_switch_level, floor_complement[1].reshape(channel_tally, lookup_extent), spike_log_decay)
    ahead = block_pass(queries, onward_lookup, memory_matrix, onward_log_decay, initial)[0]
    behind = block_pass(jnp.flip(queries, axis=0), jnp.flip(reverse_lookup, axis=0), jnp.flip(memory_matrix, axis=0), jnp.flip(reverse_log_decay, axis=0), initial)[0]
    return ahead + jnp.flip(behind, axis=0)

def reference(skip_stream, wide_probe_logits, narrow_probe_logits, wide_decay_logits, narrow_decay_logits, wide_floor_complement, narrow_floor_complement, payloads, result_switch_logits, spike_decays, channel_scale_vector, result_mapping_matrix, specialist_scale_vector, assignments, assignment_share, specialist_switch_matrix, specialist_raising_matrix, specialist_lowering_matrix):
    series_extent = skip_stream.shape[0]
    joint_heads = 3 * WIDE_GROUPS
    memory_matrix = payloads.astype(jnp.float32).reshape(series_extent, WIDE_GROUPS, 3, PAYLOAD_EXTENT)
    spike_span = spike_decays.reshape(series_extent, WIDE_GROUPS, 3)
    wide_channel_slices = twin_orientations(wide_probe_logits, wide_decay_logits, wide_floor_complement, spike_span[:, :, 0], memory_matrix[:, :, 0], WIDE_LOOKUP_WIDTH)
    narrow_channel_slices = twin_orientations(narrow_probe_logits, narrow_decay_logits, narrow_floor_complement, spike_span[:, :, 1:].reshape(series_extent, NARROW_GROUPS), memory_matrix[:, :, 1:].reshape(series_extent, NARROW_GROUPS, PAYLOAD_EXTENT), NARROW_LOOKUP)
    joined = jnp.concatenate([wide_channel_slices[:, :, None], narrow_channel_slices.reshape(series_extent, WIDE_GROUPS, 2, PAYLOAD_EXTENT)], axis=2).reshape(series_extent, joint_heads, PAYLOAD_EXTENT)
    normed_heads = joined * lax.rsqrt(lax.optimization_barrier(jnp.mean(joined * joined, axis=-1, keepdims=True)) + epsilon)
    gated_heads = normed_heads * channel_scale_vector.reshape(joint_heads, PAYLOAD_EXTENT) * jax.nn.silu(result_switch_logits.astype(jnp.float32).reshape(series_extent, joint_heads, PAYLOAD_EXTENT))
    mixed_heads = gated_heads.reshape(series_extent, joint_heads * PAYLOAD_EXTENT).astype(jnp.bfloat16)
    mixing = jnp.dot(mixed_heads, result_mapping_matrix, preferred_element_type=jnp.float32)
    hidden = (skip_stream.astype(jnp.float32) + mixing).astype(jnp.bfloat16)
    hidden_float = hidden.astype(jnp.float32)
    normed = (hidden_float * lax.rsqrt(lax.optimization_barrier(jnp.mean(hidden_float * hidden_float, axis=-1, keepdims=True)) + epsilon) * specialist_scale_vector).astype(jnp.bfloat16)
    most_rows = N_SP * N_TP * CAP
    block_total = DE // DE_PART

    def one_expert(running_sum, expert_index):
        chosen = assignments == expert_index
        weight_share = lax.optimization_barrier(jnp.sum(jnp.where(chosen, assignment_share, 0.0), axis=1))
        used_rows = jnp.any(chosen, axis=1)
        picked = jnp.nonzero(used_rows, size=most_rows, fill_value=0)[0].astype(jnp.int32)
        live_rows = jnp.arange(most_rows, dtype=jnp.int32) < jnp.sum(used_rows.astype(jnp.int32))
        gathered = normed[picked]
        gate_part = jnp.dot(gathered, specialist_switch_matrix[expert_index], preferred_element_type=jnp.float32)
        up_part = jnp.dot(gathered, specialist_raising_matrix[expert_index], preferred_element_type=jnp.float32)
        activation = (jax.nn.silu(gate_part) * up_part).astype(jnp.bfloat16)
        partial_value = jnp.einsum('mpk,pkd->mpd', activation.astype(jnp.float32).reshape(most_rows, block_total, DE_PART), specialist_lowering_matrix[expert_index].astype(jnp.float32).reshape(block_total, DE_PART, D), precision=lax.Precision.HIGHEST)
        rounded = lax.optimization_barrier(partial_value.astype(jnp.bfloat16)).astype(jnp.float32)
        expert_out = lax.optimization_barrier(jnp.sum(rounded, axis=1)).astype(jnp.bfloat16)
        row_scale = jnp.where(live_rows, weight_share[picked], 0.0)
        running_sum = running_sum.at[picked].add(row_scale[:, None] * expert_out.astype(jnp.float32))
        return (running_sum, None)
    mixture = lax.scan(one_expert, jnp.zeros((series_extent, D), jnp.float32), jnp.arange(EXPERTS, dtype=jnp.int32))[0]
    return (hidden_float + mixture).astype(jnp.bfloat16)
```

```python
import functools

import jax
import jax.numpy as jnp
from jax import lax
from jax.experimental import pallas as pl
from jax.experimental.pallas import tpu as pltpu
from jax.sharding import Mesh
from jax.sharding import PartitionSpec as P

F32 = jnp.float32
BF16 = jnp.bfloat16
EPS = 1e-06
HALF = 64
SLICE = 32
PAY = 80
CAP = 4
ZG = ("zl", "c")
SP = ("zh", "zl", "c")
GRP_SP = ("grp", "zh", "zl", "c")
GRP_SP_TP = ("grp", "zh", "zl", "c", "tp")


def dot(a, b, contract=(1, 0), precision=None):
    dims = (((contract[0],), (contract[1],)), ((), ()))
    return lax.dot_general(a, b, dims, precision=precision, preferred_element_type=F32)


def iota(shape, axis):
    return lax.broadcasted_iota(jnp.int32, shape, axis)


def split_parts(x):
    hi = x.astype(BF16)
    return hi, (x - hi.astype(F32)).astype(BF16)


def key_and_decay(logits, leaks, spikes):
    gate = jax.nn.sigmoid(-logits.astype(F32))
    rows = [leaks[d : d + 1] * gate for d in range(2)]
    return rows, [jnp.log1p(-k) + spikes for k in rows]


def scan_terms(wd, nd, wleak, nleak, spk):
    n, width = wd.shape
    spikes_w = jnp.broadcast_to(spk[:, 0:1], (n, width))
    spikes_n = jnp.where(iota((n, width), 1) < width // 2, spk[:, 1:2], spk[:, 2:3])
    kw, aw = key_and_decay(wd, wleak, spikes_w)
    kn, an = key_and_decay(nd, nleak, spikes_n)
    row, col = iota((n, n), 0), iota((n, n), 1)
    exact = lax.Precision.HIGHEST
    fwd = dot((row >= col).astype(F32), jnp.concatenate([aw[0], an[0]], axis=1), precision=exact)
    bwd = dot((row <= col).astype(F32), jnp.concatenate([aw[1], an[1]], axis=1), precision=exact)
    keys = [jnp.concatenate([kw[d], kn[d]], axis=1) for d in range(2)]
    return keys, (fwd, bwd)


def decay_rows(rows):
    width = rows[0].shape[1]
    at = iota((16, width), 0)
    block = jnp.zeros((16, width), F32)
    for n, row in enumerate(rows):
        hi = row.astype(BF16).astype(F32)
        block = jnp.where(at == 2 * n, hi, block)
        block = jnp.where(at == 2 * n + 1, row - hi, block)
    return block.astype(BF16)


def summary_kernel(wd, nd, wleak, nleak, v, spk, out):
    keys, running = scan_terms(wd[...], nd[...], wleak[...], nleak[...], spk[...])
    n, width = wd.shape
    values = v[...]
    last = (n - 1, 0)
    rows = []
    for d in range(2):
        closing = running[d][last[d] : last[d] + 1]
        fresh = (keys[d] * jnp.exp(closing - running[d])).astype(BF16)
        wide = dot(fresh[:, :width], values[:, :width], (0, 0))
        both = dot(fresh[:, width:], values[:, width:], (0, 0))
        slim = jnp.where(iota((width, width), 0) < width // 2, both[:, :width], both[:, width:])
        state = jnp.concatenate([wide, slim], axis=0).astype(BF16)
        for j in range(out.shape[0]):
            out[j, d * SLICE : (d + 1) * SLICE, :] = state[j * SLICE : (j + 1) * SLICE]
        rows += [closing[:, :width], closing[:, width:]]
    block = decay_rows(rows)
    for j in range(out.shape[0]):
        out[j, 2 * SLICE :, :] = block


def local_kernel(wp, np_, wd, nd, wleak, nleak, v, spk, o_ref, qf_ref, qb_ref):
    keys, running = scan_terms(wd[...], nd[...], wleak[...], nleak[...], spk[...])
    n, width = wd.shape
    q = jnp.concatenate(
        [
            jax.nn.silu(wp[...].astype(F32)) * width ** (-0.5),
            jax.nn.silu(np_[...].astype(F32)) * (width // 2) ** (-0.5),
        ],
        axis=1,
    )
    qf_ref[...] = (q * jnp.exp(running[0])).astype(BF16)
    qb_ref[...] = (q * jnp.exp(running[1])).astype(BF16)
    lane = iota((HALF, 2 * width), 1)
    heads = (lane < width, (lane >= width) & (lane < 3 * width // 2), lane >= 3 * width // 2)
    row, col = iota((HALF, HALF), 0), iota((HALF, HALF), 1)

    def pair(d, t, s, ref):
        rt = running[d][t * HALF : (t + 1) * HALF]
        rs = running[d][s * HALF : (s + 1) * HALF]
        base = running[d][ref : ref + 1]
        qs = q[t * HALF : (t + 1) * HALF] * jnp.exp(rt - base)
        ks = (keys[d][s * HALF : (s + 1) * HALF] * jnp.exp(base - rs)).astype(BF16)
        return qs, ks

    mid = HALF // 2
    terms = {
        (0, 0): [(0, pair(0, 0, 0, mid - 1)), (1, pair(1, 0, 0, mid))],
        (1, 1): [(0, pair(0, 1, 1, HALF + mid - 1)), (1, pair(1, 1, 1, HALF + mid))],
        (1, 0): [(None, pair(0, 1, 0, HALF - 1))],
        (0, 1): [(None, pair(1, 0, 1, HALF))],
    }

    def scores(block, head):
        total = None
        for d, (qs, ks) in terms[block]:
            lo = 0 if head == 0 else width
            picked = jnp.where(heads[head], qs, 0.0)[:, lo : lo + width].astype(BF16)
            part = dot(picked, ks[:, lo : lo + width], (1, 1))
            if d is not None:
                part = jnp.where(row >= col if d == 0 else row <= col, part, 0.0)
            total = part if total is None else total + part
        return total

    for head in range(3):
        full = jnp.concatenate(
            [
                jnp.concatenate([scores((0, 0), head), scores((0, 1), head)], axis=1),
                jnp.concatenate([scores((1, 0), head), scores((1, 1), head)], axis=1),
            ],
            axis=0,
        ).astype(BF16)
        at = slice(head * width, (head + 1) * width)
        o_ref[:, at] = dot(full, v[:, at])


def pick_column(block, d, member):
    width = block.shape[1]
    per = width // SLICE
    rows = block.astype(F32)
    wide = rows[4 * d : 4 * d + 1] + rows[4 * d + 1 : 4 * d + 2]
    slim = rows[4 * d + 2 : 4 * d + 3] + rows[4 * d + 3 : 4 * d + 4]
    row = jnp.where(member >= per, slim, wide)
    want = iota((SLICE, width), 0) + SLICE * (member % per)
    hit = iota((SLICE, width), 1) == want
    return jnp.sum(jnp.where(hit, row, 0.0), axis=1, keepdims=True)


def group_kernel(place, got, pre_ref, dec_ref, tot_ref):
    member = place[1]
    count, _, width = got.shape
    summed = jnp.zeros((16, width), F32)
    for i in range(count):
        summed = summed + got[i, 2 * SLICE :, :].astype(F32)
    for d in range(2):
        at = slice(d * SLICE, (d + 1) * SLICE)
        state = jnp.zeros((SLICE, width), F32)
        total = jnp.zeros((SLICE, 1), F32)
        for i in range(count) if d == 0 else reversed(range(count)):
            pre_ref[i, at, :] = state
            dec_ref[i, at, :] = jnp.broadcast_to(jnp.exp(total), (SLICE, width))
            column = pick_column(got[i, 2 * SLICE :, :], d, member)
            state = jnp.exp(column) * state + got[i, at, :].astype(F32)
            total = total + column
        tot_ref[at, :] = state.astype(BF16)
    rows = [summed[2 * n : 2 * n + 1] + summed[2 * n + 1 : 2 * n + 2] for n in range(4)]
    tot_ref[2 * SLICE :, :] = decay_rows(rows)


def carry_kernel(place, r1, r2, r3, pre, dec, out):
    group, member, groups = place[0], place[1], place[2]
    count, _, width = pre.shape
    came = {1: r1, 2: r2, 3: r3}
    for d in range(2):
        at = slice(d * SLICE, (d + 1) * SLICE)
        carry = jnp.zeros((SLICE, width), F32)
        for back in (3, 2, 1):
            ref = came[back] if d == 0 else came[4 - back]
            live = group - back >= 0 if d == 0 else group + back < groups
            column = pick_column(ref[2 * SLICE :, :], d, member)
            moved = jnp.exp(column) * carry + ref[at, :].astype(F32)
            carry = jnp.where(live, moved, carry)
        for i in range(count):
            out[i, at, :] = (pre[i, at, :] + dec[i, at, :] * carry).astype(BF16)


def mix_kernel(states, o_ref, qf, qb, gate, gain, proj, out):
    n, width = o_ref.shape[0], states.shape[2]
    members = states.shape[0]
    entering = [
        jnp.concatenate(
            [states[j, d * SLICE : (d + 1) * SLICE, :] for j in range(members)], axis=0
        )
        for d in range(2)
    ]
    low = iota((n, width), 1) < width // 2
    mixed = []
    for head in range(3):
        at = slice(head * width, (head + 1) * width)
        total = o_ref[:, at]
        for d, q in enumerate((qf, qb)):
            if head == 0:
                total = total + dot(q[:, :width], entering[d][:width])
            else:
                keep = low if head == 1 else jnp.logical_not(low)
                own = jnp.where(keep, q[:, width:].astype(F32), 0.0).astype(BF16)
                total = total + dot(own, entering[d][width:])
        total = total * lax.rsqrt(jnp.mean(total * total, axis=1, keepdims=True) + EPS)
        total = total * gain[:, at] * jax.nn.silu(gate[:, at].astype(F32))
        mixed.append(total.astype(BF16))
    out[...] = dot(jnp.concatenate(mixed, axis=1), proj[...]).astype(BF16)


def slot_matrix(routes):
    rows = routes.shape[1]
    slots = 32 * CAP
    expert = iota((slots, rows), 0) // CAP
    first = routes[0:1] == expert
    second = routes[1:2] == expert
    named = jnp.logical_or(first, second)
    before = (iota((rows, rows), 0) < iota((rows, rows), 1)).astype(F32).astype(BF16)
    rank = dot(named.astype(F32).astype(BF16), before)
    placed = rank.astype(jnp.int32) == iota((slots, rows), 0) % CAP
    return jnp.logical_and(first, placed), jnp.logical_and(second, placed)


def dispatch_kernel(parts, skip, gain, routes, hidden_ref, out):
    mixing = parts[0].astype(F32)
    for k in range(1, parts.shape[0]):
        mixing = mixing + parts[k].astype(F32)
    hidden_bf = (skip[...].astype(F32) + mixing).astype(BF16)
    hidden_ref[...] = hidden_bf
    hidden = hidden_bf.astype(F32)
    normed = hidden * lax.rsqrt(jnp.mean(hidden * hidden, axis=1, keepdims=True) + EPS)
    normed = (normed * gain[...]).astype(BF16)
    first, second = slot_matrix(routes[...])
    chosen = jnp.logical_or(first, second).astype(F32).astype(BF16)
    out[...] = dot(chosen, normed).astype(BF16)


def expert_kernel(count, *refs):
    rows, (wg, wu, wd), outs, acc = refs[:count], refs[count : count + 3], refs[count + 3 : -1], refs[-1]
    step = pl.program_id(0)
    x = rows[0][...] if count == 1 else jnp.concatenate([r[...] for r in rows], axis=0)
    up = dot(x, wu[...])
    act = (jax.nn.silu(dot(x, wg[...])) * up).astype(BF16)
    part = dot(act, wd[...])

    @pl.when(step == 0)
    def _():
        acc[...] = part

    @pl.when(step > 0)
    def _():
        acc[...] += part

    @pl.when(step == pl.num_programs(0) - 1)
    def _():
        size = outs[0].shape[0]
        for k, out in enumerate(outs):
            out[...] = acc[k * size : (k + 1) * size].astype(BF16)


def expert_parts(rows, wg, wu, wd, piece):
    width, hidden = wg.shape
    block = 128
    total = sum(r.shape[0] for r in rows)
    whole = lambda r: pl.BlockSpec(r, lambda i: (0, 0))
    out = jax.ShapeDtypeStruct((piece, width), BF16)
    return pl.pallas_call(
        functools.partial(expert_kernel, len(rows)),
        grid=(hidden // block,),
        in_specs=[whole(r.shape) for r in rows]
        + [
            pl.BlockSpec((width, block), lambda i: (0, i)),
            pl.BlockSpec((width, block), lambda i: (0, i)),
            pl.BlockSpec((block, width), lambda i: (i, 0)),
        ],
        out_specs=[whole((piece, width))] * (total // piece),
        out_shape=[out] * (total // piece),
        scratch_shapes=[pltpu.VMEM((total, width), F32)],
        cost_estimate=pl.CostEstimate(
            flops=6 * total * width * hidden,
            bytes_accessed=6 * width * hidden,
            transcendentals=total * hidden,
        ),
    )(*rows, wg, wu, wd)


def combine_kernel(hidden, back, routes, share, out):
    first, second = slot_matrix(routes[...])
    weight = jnp.where(first, share[0:1], 0.0) + jnp.where(second, share[1:2], 0.0)
    hi, lo = split_parts(weight)
    rows = back[...]
    mixture = dot(hi, rows, (0, 0)) + dot(lo, rows, (0, 0))
    out[...] = (hidden[...].astype(F32) + mixture).astype(BF16)


def sds(shape, dtype):
    return jax.ShapeDtypeStruct(shape, dtype)


VMEM = pl.BlockSpec(memory_space=pltpu.VMEM)
SMEM = pl.BlockSpec(memory_space=pltpu.SMEM)


def cost(flops):
    return pl.CostEstimate(flops=flops, bytes_accessed=1 << 20, transcendentals=0)


def local(
    skip_stream,
    wide_probe_logits,
    narrow_probe_logits,
    wide_decay_logits,
    narrow_decay_logits,
    wide_floor_complement,
    narrow_floor_complement,
    payloads,
    result_switch_logits,
    spike_decays,
    channel_scale_vector,
    result_mapping_matrix,
    specialist_scale_vector,
    assignments,
    assignment_share,
    specialist_switch_matrix,
    specialist_raising_matrix,
    specialist_lowering_matrix,
):
    tokens, width = wide_probe_logits.shape
    rows, model = skip_stream.shape
    joint = payloads.shape[1]
    members = lax.axis_size(ZG)
    groups = lax.axis_size("zh")
    shards = lax.axis_size("tp")
    experts = lax.axis_size(SP)
    place = jnp.stack(
        [lax.axis_index("zh"), lax.axis_index(ZG), jnp.int32(groups)]
    ).astype(jnp.int32)
    decay_args = (
        wide_decay_logits,
        narrow_decay_logits,
        wide_floor_complement,
        narrow_floor_complement,
        payloads,
        spike_decays,
    )

    summary = pl.pallas_call(
        summary_kernel, out_shape=sds((members, PAY, width), BF16), cost_estimate=cost(4 << 20)
    )(*decay_args)
    by_slice = lax.all_to_all(summary, ZG, 0, 0, tiled=True)
    inside, q_fwd, q_bwd = pl.pallas_call(
        local_kernel,
        out_shape=[
            sds((tokens, joint), F32),
            sds((tokens, 2 * width), BF16),
            sds((tokens, 2 * width), BF16),
        ],
        cost_estimate=cost(64 << 20),
    )(wide_probe_logits, narrow_probe_logits, *decay_args)
    before, decayed, total = pl.pallas_call(
        group_kernel,
        in_specs=[SMEM, VMEM],
        out_shape=[
            sds((members, 2 * SLICE, width), F32),
            sds((members, 2 * SLICE, width), F32),
            sds((PAY, width), BF16),
        ],
        cost_estimate=cost(4 << 20),
    )(place, by_slice)
    came = [
        lax.ppermute(total, "zh", [(i, (i + k) % groups) for i in range(groups)])
        for k in (1, 2, 3)
    ]
    carried = pl.pallas_call(
        carry_kernel,
        in_specs=[SMEM] + [VMEM] * 5,
        out_shape=sds((members, 2 * SLICE, width), BF16),
        cost_estimate=cost(4 << 20),
    )(place, *came, before, decayed)
    entering = lax.all_to_all(carried, ZG, 0, 0, tiled=True)
    mixed = pl.pallas_call(
        mix_kernel, out_shape=sds((tokens, model), BF16), cost_estimate=cost(256 << 20)
    )(
        entering,
        inside,
        q_fwd,
        q_bwd,
        result_switch_logits,
        channel_scale_vector.reshape(1, joint),
        result_mapping_matrix,
    )
    parts = lax.all_to_all(mixed.reshape(shards, rows, model), "tp", 0, 0, tiled=True)
    routes = assignments.T
    share = assignment_share.T
    slots = experts * CAP
    hidden, outgoing = pl.pallas_call(
        dispatch_kernel,
        out_shape=[sds((rows, model), BF16), sds((slots, model), BF16)],
        cost_estimate=cost(16 << 20),
    )(parts, skip_stream, specialist_scale_vector.reshape(1, model), routes)
    own = lax.all_to_all(outgoing.reshape(experts, CAP, model), SP, 0, 0, tiled=True)
    own = own.reshape(slots, model)

    up_ring = [(i, (i + 1) % shards) for i in range(shards)]
    down_ring = [(i, (i - 1) % shards) for i in range(shards)]
    up = lambda x: lax.ppermute(x, "tp", up_ring)
    down = lambda x: lax.ppermute(x, "tp", down_ring)
    half = slots // 2
    weights = (
        specialist_switch_matrix[0],
        specialist_raising_matrix[0],
        specialist_lowering_matrix[0],
    )
    from_left, from_right = up(own), down(own)
    far_low, far_high = up(from_left[:half]), down(from_right[half:])
    (own_part,) = expert_parts([own], *weights, slots)
    left_low, left_high, right_low, right_high = expert_parts(
        [from_left, from_right], *weights, half
    )
    left_got_high = up(right_high)
    right_got_low = down(left_low)
    opp_low, opp_high = expert_parts([far_low, far_high], *weights, half)
    add_low, add_high = up(opp_low), down(opp_high)
    joined = lambda a, b: (a.astype(F32) + b.astype(F32)).astype(BF16)
    left_got_low = up(joined(right_low, add_low))
    right_got_high = down(joined(left_high, add_high))
    f = lambda x: x.astype(F32)
    summed = jnp.concatenate(
        [
            (f(own_part[:half]) + f(left_got_low) + f(right_got_low)).astype(BF16),
            (f(own_part[half:]) + f(left_got_high) + f(right_got_high)).astype(BF16),
        ],
        axis=0,
    )
    back = lax.all_to_all(summed.reshape(experts, CAP, model), SP, 0, 0, tiled=True)
    return pl.pallas_call(
        combine_kernel, out_shape=sds((rows, model), BF16), cost_estimate=cost(16 << 20)
    )(hidden, back.reshape(slots, model), routes, share)


def solution(mesh):
    torus = Mesh(
        mesh.devices.reshape(mesh.shape["grp"], 4, 4, 2, mesh.shape["tp"]),
        GRP_SP_TP,
    )
    placed = (
        P(GRP_SP_TP, None),
        P(GRP_SP, "tp"),
        P(GRP_SP, "tp"),
        P(GRP_SP, "tp"),
        P(GRP_SP, "tp"),
        P(None, "tp"),
        P(None, "tp"),
        P(GRP_SP, "tp"),
        P(GRP_SP, "tp"),
        P(GRP_SP, "tp"),
        P("tp"),
        P("tp", None),
        P(),
        P(GRP_SP_TP, None),
        P(GRP_SP_TP, None),
        P(SP, None, "tp"),
        P(SP, None, "tp"),
        P(SP, "tp", None),
    )
    return jax.shard_map(
        local, mesh=torus, in_specs=placed, out_specs=P(GRP_SP_TP, None), check_vma=False
    )
```

```python
import jax
import jax.numpy as jnp
from jax import lax
from jax.experimental import pallas as pl
from jax.experimental.pallas import tpu as pltpu
from jax.sharding import Mesh
from jax.sharding import PartitionSpec as P

F32 = jnp.float32
BF16 = jnp.bfloat16
EPS = 1e-06
HALF = 64
SLICE = 32
PAY = 80
CAP = 4
ZG = ("zl", "c")
SP = ("zh", "zl", "c")
GRP_SP = ("grp", "zh", "zl", "c")
GRP_SP_TP = ("grp", "zh", "zl", "c", "tp")


def dot(a, b, contract=(1, 0), precision=None):
    dims = (((contract[0],), (contract[1],)), ((), ()))
    return lax.dot_general(a, b, dims, precision=precision, preferred_element_type=F32)


def iota(shape, axis):
    return lax.broadcasted_iota(jnp.int32, shape, axis)


def split_parts(x):
    hi = x.astype(BF16)
    return hi, (x - hi.astype(F32)).astype(BF16)


def key_and_decay(logits, leaks, spikes):
    gate = jax.nn.sigmoid(-logits.astype(F32))
    rows = [leaks[d : d + 1] * gate for d in range(2)]
    return rows, [jnp.log1p(-k) + spikes for k in rows]


def scan_terms(wd, nd, wleak, nleak, spk):
    n, width = wd.shape
    exact = lax.Precision.HIGHEST
    heads = spk.shape[0]
    lane = iota((heads, 2 * width), 1)
    owner = jnp.where(lane < width, 0, jnp.where(lane < 3 * width // 2, 1, 2))
    spikes = dot(spk, (iota((heads, 2 * width), 0) == owner).astype(F32), (0, 0), exact)
    kw, aw = key_and_decay(wd, wleak, spikes[:, :width])
    kn, an = key_and_decay(nd, nleak, spikes[:, width:])
    row, col = iota((n, n), 0), iota((n, n), 1)
    fwd = dot((row >= col).astype(F32), jnp.concatenate([aw[0], an[0]], axis=1), precision=exact)
    bwd = dot((row <= col).astype(F32), jnp.concatenate([aw[1], an[1]], axis=1), precision=exact)
    keys = [jnp.concatenate([kw[d], kn[d]], axis=1) for d in range(2)]
    return keys, (fwd, bwd)


def decay_rows(rows):
    width = rows[0].shape[1]
    at = iota((16, width), 0)
    block = jnp.zeros((16, width), F32)
    for n, row in enumerate(rows):
        hi = row.astype(BF16).astype(F32)
        block = jnp.where(at == 2 * n, hi, block)
        block = jnp.where(at == 2 * n + 1, row - hi, block)
    return block.astype(BF16)


def summary_kernel(wd, nd, wleak, nleak, v, spk, out):
    keys, running = scan_terms(wd[...], nd[...], wleak[...], nleak[...], spk[...])
    n, width = wd.shape
    values = v[...]
    last = (n - 1, 0)
    rows = []
    for d in range(2):
        closing = running[d][last[d] : last[d] + 1]
        fresh = (keys[d] * jnp.exp(closing - running[d])).astype(BF16)
        wide = dot(fresh[:, :width], values[:, :width], (0, 0))
        both = dot(fresh[:, width:], values[:, width:], (0, 0))
        slim = jnp.where(iota((width, width), 0) < width // 2, both[:, :width], both[:, width:])
        state = jnp.concatenate([wide, slim], axis=0).astype(BF16)
        for j in range(out.shape[0]):
            out[j, d * SLICE : (d + 1) * SLICE, :] = state[j * SLICE : (j + 1) * SLICE]
        rows += [closing[:, :width], closing[:, width:]]
    block = decay_rows(rows)
    for j in range(out.shape[0]):
        out[j, 2 * SLICE :, :] = block


def local_kernel(wp, np_, wd, nd, wleak, nleak, v, spk, o_ref, qf_ref, qb_ref):
    keys, running = scan_terms(wd[...], nd[...], wleak[...], nleak[...], spk[...])
    _, width = wd.shape
    q = jnp.concatenate(
        [
            jax.nn.silu(wp[...].astype(F32)) * width ** (-0.5),
            jax.nn.silu(np_[...].astype(F32)) * (width // 2) ** (-0.5),
        ],
        axis=1,
    )
    qf_ref[...] = (q * jnp.exp(running[0])).astype(BF16)
    qb_ref[...] = (q * jnp.exp(running[1])).astype(BF16)
    lane = iota((HALF, 2 * width), 1)
    heads = (lane < width, (lane >= width) & (lane < 3 * width // 2), lane >= 3 * width // 2)
    row, col = iota((HALF, HALF), 0), iota((HALF, HALF), 1)

    def pair(d, t, s, ref):
        rt = running[d][t * HALF : (t + 1) * HALF]
        rs = running[d][s * HALF : (s + 1) * HALF]
        base = running[d][ref : ref + 1]
        qs = q[t * HALF : (t + 1) * HALF] * jnp.exp(rt - base)
        ks = (keys[d][s * HALF : (s + 1) * HALF] * jnp.exp(base - rs)).astype(BF16)
        return qs, ks

    mid = HALF // 2
    terms = {
        (0, 0): [(0, pair(0, 0, 0, mid - 1)), (1, pair(1, 0, 0, mid))],
        (1, 1): [(0, pair(0, 1, 1, HALF + mid - 1)), (1, pair(1, 1, 1, HALF + mid))],
        (1, 0): [(None, pair(0, 1, 0, HALF - 1))],
        (0, 1): [(None, pair(1, 0, 1, HALF))],
    }

    def scores(block, head):
        total = None
        for d, (qs, ks) in terms[block]:
            lo = 0 if head == 0 else width
            picked = jnp.where(heads[head], qs, 0.0)[:, lo : lo + width].astype(BF16)
            part = dot(picked, ks[:, lo : lo + width], (1, 1))
            if d is not None:
                part = jnp.where(row >= col if d == 0 else row <= col, part, 0.0)
            total = part if total is None else total + part
        return total

    for head in range(3):
        full = jnp.concatenate(
            [
                jnp.concatenate([scores((0, 0), head), scores((0, 1), head)], axis=1),
                jnp.concatenate([scores((1, 0), head), scores((1, 1), head)], axis=1),
            ],
            axis=0,
        ).astype(BF16)
        at = slice(head * width, (head + 1) * width)
        o_ref[:, at] = dot(full, v[:, at])


def pick_column(block, d, member):
    width = block.shape[1]
    per = width // SLICE
    rows = block.astype(F32)
    wide = rows[4 * d : 4 * d + 1] + rows[4 * d + 1 : 4 * d + 2]
    slim = rows[4 * d + 2 : 4 * d + 3] + rows[4 * d + 3 : 4 * d + 4]
    row = jnp.where(member >= per, slim, wide)
    want = iota((SLICE, width), 0) + SLICE * (member % per)
    hit = iota((SLICE, width), 1) == want
    return jnp.sum(jnp.where(hit, row, 0.0), axis=1, keepdims=True)


def group_kernel(place, got, pre_ref, dec_ref, tot_ref):
    member = place[1]
    count, _, width = got.shape
    summed = jnp.zeros((16, width), F32)
    for i in range(count):
        summed = summed + got[i, 2 * SLICE :, :].astype(F32)
    for d in range(2):
        at = slice(d * SLICE, (d + 1) * SLICE)
        state = jnp.zeros((SLICE, width), F32)
        total = jnp.zeros((SLICE, 1), F32)
        for i in range(count) if d == 0 else reversed(range(count)):
            pre_ref[i, at, :] = state
            dec_ref[i, at, :] = jnp.broadcast_to(jnp.exp(total), (SLICE, width))
            column = pick_column(got[i, 2 * SLICE :, :], d, member)
            state = jnp.exp(column) * state + got[i, at, :].astype(F32)
            total = total + column
        tot_ref[at, :] = state.astype(BF16)
    rows = [summed[2 * n : 2 * n + 1] + summed[2 * n + 1 : 2 * n + 2] for n in range(4)]
    tot_ref[2 * SLICE :, :] = decay_rows(rows)


def carry_kernel(place, r1, r2, r3, pre, dec, out):
    group, member, groups = place[0], place[1], place[2]
    count, _, width = pre.shape
    came = {1: r1, 2: r2, 3: r3}
    for d in range(2):
        at = slice(d * SLICE, (d + 1) * SLICE)
        carry = jnp.zeros((SLICE, width), F32)
        for back in (3, 2, 1):
            ref = came[back] if d == 0 else came[4 - back]
            live = group - back >= 0 if d == 0 else group + back < groups
            column = pick_column(ref[2 * SLICE :, :], d, member)
            moved = jnp.exp(column) * carry + ref[at, :].astype(F32)
            carry = jnp.where(live, moved, carry)
        for i in range(count):
            out[i, at, :] = (pre[i, at, :] + dec[i, at, :] * carry).astype(BF16)


def mix_kernel(states, o_ref, qf, qb, gate, gain, proj, out):
    n, width = o_ref.shape[0], states.shape[2]
    members = states.shape[0]
    entering = [
        jnp.concatenate(
            [states[j, d * SLICE : (d + 1) * SLICE, :] for j in range(members)], axis=0
        )
        for d in range(2)
    ]
    low = iota((n, width), 1) < width // 2
    mixed = []
    for head in range(3):
        at = slice(head * width, (head + 1) * width)
        total = o_ref[:, at]
        for d, q in enumerate((qf, qb)):
            if head == 0:
                total = total + dot(q[:, :width], entering[d][:width])
            else:
                keep = low if head == 1 else jnp.logical_not(low)
                own = jnp.where(keep, q[:, width:].astype(F32), 0.0).astype(BF16)
                total = total + dot(own, entering[d][width:])
        total = total * lax.rsqrt(jnp.mean(total * total, axis=1, keepdims=True) + EPS)
        total = total * gain[:, at] * jax.nn.silu(gate[:, at].astype(F32))
        mixed.append(total.astype(BF16))
    out[...] = dot(jnp.concatenate(mixed, axis=1), proj[...]).astype(BF16)


def slot_matrix(routes):
    rows = routes.shape[1]
    slots = 32 * CAP
    expert = iota((slots, rows), 0) // CAP
    first = routes[0:1] == expert
    second = routes[1:2] == expert
    named = jnp.logical_or(first, second)
    before = (iota((rows, rows), 0) < iota((rows, rows), 1)).astype(F32).astype(BF16)
    rank = dot(named.astype(F32).astype(BF16), before)
    placed = rank.astype(jnp.int32) == iota((slots, rows), 0) % CAP
    return jnp.logical_and(first, placed), jnp.logical_and(second, placed)


def dispatch_kernel(parts, skip, gain, routes, hidden_ref, out):
    mixing = parts[0].astype(F32)
    for k in range(1, parts.shape[0]):
        mixing = mixing + parts[k].astype(F32)
    hidden_bf = (skip[...].astype(F32) + mixing).astype(BF16)
    hidden_ref[...] = hidden_bf
    hidden = hidden_bf.astype(F32)
    normed = hidden * lax.rsqrt(jnp.mean(hidden * hidden, axis=1, keepdims=True) + EPS)
    normed = (normed * gain[...]).astype(BF16)
    first, second = slot_matrix(routes[...])
    chosen = jnp.logical_or(first, second).astype(F32).astype(BF16)
    out[...] = dot(chosen, normed).astype(BF16)


def expert_part(rows, wg, wu, wd):
    gate = jnp.dot(rows, wg, preferred_element_type=F32)
    up = jnp.dot(rows, wu, preferred_element_type=F32)
    act = (jax.nn.silu(gate) * up).astype(BF16)
    return jnp.dot(act, wd, preferred_element_type=F32).astype(BF16)


def combine_kernel(hidden, back, routes, share, out):
    first, second = slot_matrix(routes[...])
    weight = jnp.where(first, share[0:1], 0.0) + jnp.where(second, share[1:2], 0.0)
    hi, lo = split_parts(weight)
    rows = back[...]
    mixture = dot(hi, rows, (0, 0)) + dot(lo, rows, (0, 0))
    out[...] = (hidden[...].astype(F32) + mixture).astype(BF16)


def sds(shape, dtype):
    return jax.ShapeDtypeStruct(shape, dtype)


VMEM = pl.BlockSpec(memory_space=pltpu.VMEM)
SMEM = pl.BlockSpec(memory_space=pltpu.SMEM)


def cost(flops):
    return pl.CostEstimate(flops=flops, bytes_accessed=1 << 20, transcendentals=0)


def local(
    skip_stream,
    wide_probe_logits,
    narrow_probe_logits,
    wide_decay_logits,
    narrow_decay_logits,
    wide_floor_complement,
    narrow_floor_complement,
    payloads,
    result_switch_logits,
    spike_decays,
    channel_scale_vector,
    result_mapping_matrix,
    specialist_scale_vector,
    assignments,
    assignment_share,
    specialist_switch_matrix,
    specialist_raising_matrix,
    specialist_lowering_matrix,
):
    tokens, width = wide_probe_logits.shape
    rows, model = skip_stream.shape
    joint = payloads.shape[1]
    members = lax.axis_size(ZG)
    groups = lax.axis_size("zh")
    shards = lax.axis_size("tp")
    experts = lax.axis_size(SP)
    place = jnp.stack(
        [lax.axis_index("zh"), lax.axis_index(ZG), jnp.int32(groups)]
    ).astype(jnp.int32)
    decay_args = (
        wide_decay_logits,
        narrow_decay_logits,
        wide_floor_complement,
        narrow_floor_complement,
        payloads,
        spike_decays.T,
    )

    summary = pl.pallas_call(
        summary_kernel, out_shape=sds((members, PAY, width), BF16), cost_estimate=cost(4 << 20)
    )(*decay_args)
    by_slice = lax.all_to_all(summary, ZG, 0, 0, tiled=True)
    inside, q_fwd, q_bwd = pl.pallas_call(
        local_kernel,
        out_shape=[
            sds((tokens, joint), F32),
            sds((tokens, 2 * width), BF16),
            sds((tokens, 2 * width), BF16),
        ],
        cost_estimate=cost(64 << 20),
    )(wide_probe_logits, narrow_probe_logits, *decay_args)
    before, decayed, total = pl.pallas_call(
        group_kernel,
        in_specs=[SMEM, VMEM],
        out_shape=[
            sds((members, 2 * SLICE, width), F32),
            sds((members, 2 * SLICE, width), F32),
            sds((PAY, width), BF16),
        ],
        cost_estimate=cost(4 << 20),
    )(place, by_slice)
    came = [
        lax.ppermute(total, "zh", [(i, (i + k) % groups) for i in range(groups)])
        for k in (1, 2, 3)
    ]
    carried = pl.pallas_call(
        carry_kernel,
        in_specs=[SMEM] + [VMEM] * 5,
        out_shape=sds((members, 2 * SLICE, width), BF16),
        cost_estimate=cost(4 << 20),
    )(place, *came, before, decayed)
    entering = lax.all_to_all(carried, ZG, 0, 0, tiled=True)
    mixed = pl.pallas_call(
        mix_kernel, out_shape=sds((tokens, model), BF16), cost_estimate=cost(256 << 20)
    )(
        entering,
        inside,
        q_fwd,
        q_bwd,
        result_switch_logits,
        channel_scale_vector.reshape(1, joint),
        result_mapping_matrix,
    )
    parts = lax.all_to_all(mixed.reshape(shards, rows, model), "tp", 0, 0, tiled=True)
    routes = assignments.T
    share = assignment_share.T
    slots = experts * CAP
    hidden, outgoing = pl.pallas_call(
        dispatch_kernel,
        out_shape=[sds((rows, model), BF16), sds((slots, model), BF16)],
        cost_estimate=cost(16 << 20),
    )(parts, skip_stream, specialist_scale_vector.reshape(1, model), routes)
    own = lax.all_to_all(outgoing.reshape(experts, CAP, model), SP, 0, 0, tiled=True)
    own = own.reshape(slots, model)

    up_ring = [(i, (i + 1) % shards) for i in range(shards)]
    down_ring = [(i, (i - 1) % shards) for i in range(shards)]
    up = lambda x: lax.ppermute(x, "tp", up_ring)
    down = lambda x: lax.ppermute(x, "tp", down_ring)
    half = slots // 2
    weights = (
        specialist_switch_matrix[0],
        specialist_raising_matrix[0],
        specialist_lowering_matrix[0],
    )
    hold = lax.optimization_barrier
    from_left = up(own)
    from_right = down(own)
    own_part = expert_part(own, *weights)
    from_left, from_right, own_part = hold((from_left, from_right, own_part))
    far_low = up(from_left[:half])
    far_high = down(from_right[half:])
    left_part = expert_part(from_left, *weights)
    right_part = expert_part(from_right, *weights)
    far_low, far_high, left_part, right_part = hold((far_low, far_high, left_part, right_part))
    left_got_high = up(right_part[half:])
    right_got_low = down(left_part[:half])
    opposite = expert_part(jnp.concatenate([far_low, far_high], axis=0), *weights)
    add_low, add_high = up(opposite[:half]), down(opposite[half:])
    joined = lambda a, b: (a.astype(F32) + b.astype(F32)).astype(BF16)
    left_got_low = up(joined(right_part[:half], add_low))
    right_got_high = down(joined(left_part[half:], add_high))
    f = lambda x: x.astype(F32)
    summed = jnp.concatenate(
        [
            (f(own_part[:half]) + f(left_got_low) + f(right_got_low)).astype(BF16),
            (f(own_part[half:]) + f(left_got_high) + f(right_got_high)).astype(BF16),
        ],
        axis=0,
    )
    back = lax.all_to_all(summed.reshape(experts, CAP, model), SP, 0, 0, tiled=True)
    return pl.pallas_call(
        combine_kernel, out_shape=sds((rows, model), BF16), cost_estimate=cost(16 << 20)
    )(hidden, back.reshape(slots, model), routes, share)


def solution(mesh):
    torus = Mesh(
        mesh.devices.reshape(mesh.shape["grp"], 4, 4, 2, mesh.shape["tp"]),
        GRP_SP_TP,
    )
    placed = (
        P(GRP_SP_TP, None),
        P(GRP_SP, "tp"),
        P(GRP_SP, "tp"),
        P(GRP_SP, "tp"),
        P(GRP_SP, "tp"),
        P(None, "tp"),
        P(None, "tp"),
        P(GRP_SP, "tp"),
        P(GRP_SP, "tp"),
        P(GRP_SP, "tp"),
        P("tp"),
        P("tp", None),
        P(),
        P(GRP_SP_TP, None),
        P(GRP_SP_TP, None),
        P(SP, None, "tp"),
        P(SP, None, "tp"),
        P(SP, "tp", None),
    )
    return jax.shard_map(
        local, mesh=torus, in_specs=placed, out_specs=P(GRP_SP_TP, None), check_vma=False
    )
```

```python
import jax
import jax.numpy as jnp
from jax import lax
from jax.experimental import pallas as pl
from jax.experimental.pallas import tpu as pltpu
from jax.sharding import Mesh
from jax.sharding import PartitionSpec as P

F32 = jnp.float32
BF16 = jnp.bfloat16
EPS = 1e-06
HALF = 64
SLICE = 32
PAY = 80
CAP = 4
ZG = ("zl", "c")
SP = ("zh", "zl", "c")
GRP_SP = ("grp", "zh", "zl", "c")
GRP_SP_TP = ("grp", "zh", "zl", "c", "tp")


def dot(a, b, contract=(1, 0), precision=None):
    dims = (((contract[0],), (contract[1],)), ((), ()))
    return lax.dot_general(a, b, dims, precision=precision, preferred_element_type=F32)


def iota(shape, axis):
    return lax.broadcasted_iota(jnp.int32, shape, axis)


def split_parts(x):
    hi = x.astype(BF16)
    return hi, (x - hi.astype(F32)).astype(BF16)


def key_and_decay(logits, leaks, spikes):
    gate = jax.nn.sigmoid(-logits.astype(F32))
    rows = [leaks[d : d + 1] * gate for d in range(2)]
    return rows, [jnp.log1p(-k) + spikes for k in rows]


def scan_terms(wd, nd, wleak, nleak, spk):
    n, width = wd.shape
    exact = lax.Precision.HIGHEST
    heads = spk.shape[0]
    lane = iota((heads, 2 * width), 1)
    owner = jnp.where(lane < width, 0, jnp.where(lane < 3 * width // 2, 1, 2))
    spikes = dot(spk, (iota((heads, 2 * width), 0) == owner).astype(F32), (0, 0), exact)
    kw, aw = key_and_decay(wd, wleak, spikes[:, :width])
    kn, an = key_and_decay(nd, nleak, spikes[:, width:])
    row, col = iota((n, n), 0), iota((n, n), 1)
    fwd = dot((row >= col).astype(F32), jnp.concatenate([aw[0], an[0]], axis=1), precision=exact)
    bwd = dot((row <= col).astype(F32), jnp.concatenate([aw[1], an[1]], axis=1), precision=exact)
    keys = [jnp.concatenate([kw[d], kn[d]], axis=1) for d in range(2)]
    return keys, (fwd, bwd)


def decay_rows(rows):
    width = rows[0].shape[1]
    at = iota((16, width), 0)
    block = jnp.zeros((16, width), F32)
    for n, row in enumerate(rows):
        hi = row.astype(BF16).astype(F32)
        block = jnp.where(at == 2 * n, hi, block)
        block = jnp.where(at == 2 * n + 1, row - hi, block)
    return block.astype(BF16)


def summary_kernel(wd, nd, wleak, nleak, v, spk, out):
    keys, running = scan_terms(wd[...], nd[...], wleak[...], nleak[...], spk[...])
    n, width = wd.shape
    values = v[...]
    last = (n - 1, 0)
    rows = []
    for d in range(2):
        closing = running[d][last[d] : last[d] + 1]
        fresh = (keys[d] * jnp.exp(closing - running[d])).astype(BF16)
        wide = dot(fresh[:, :width], values[:, :width], (0, 0))
        both = dot(fresh[:, width:], values[:, width:], (0, 0))
        slim = jnp.where(iota((width, width), 0) < width // 2, both[:, :width], both[:, width:])
        state = jnp.concatenate([wide, slim], axis=0).astype(BF16)
        for j in range(out.shape[0]):
            out[j, d * SLICE : (d + 1) * SLICE, :] = state[j * SLICE : (j + 1) * SLICE]
        rows += [closing[:, :width], closing[:, width:]]
    block = decay_rows(rows)
    for j in range(out.shape[0]):
        out[j, 2 * SLICE :, :] = block


def local_kernel(wp, np_, wd, nd, wleak, nleak, v, spk, o_ref, qf_ref, qb_ref):
    keys, running = scan_terms(wd[...], nd[...], wleak[...], nleak[...], spk[...])
    _, width = wd.shape
    q = jnp.concatenate(
        [
            jax.nn.silu(wp[...].astype(F32)) * width ** (-0.5),
            jax.nn.silu(np_[...].astype(F32)) * (width // 2) ** (-0.5),
        ],
        axis=1,
    )
    qf_ref[...] = (q * jnp.exp(running[0])).astype(BF16)
    qb_ref[...] = (q * jnp.exp(running[1])).astype(BF16)
    lane = iota((HALF, 2 * width), 1)
    heads = (lane < width, (lane >= width) & (lane < 3 * width // 2), lane >= 3 * width // 2)
    row, col = iota((HALF, HALF), 0), iota((HALF, HALF), 1)

    def pair(d, t, s, ref):
        rt = running[d][t * HALF : (t + 1) * HALF]
        rs = running[d][s * HALF : (s + 1) * HALF]
        base = running[d][ref : ref + 1]
        qs = q[t * HALF : (t + 1) * HALF] * jnp.exp(rt - base)
        ks = (keys[d][s * HALF : (s + 1) * HALF] * jnp.exp(base - rs)).astype(BF16)
        return qs, ks

    mid = HALF // 2
    terms = {
        (0, 0): [(0, pair(0, 0, 0, mid - 1)), (1, pair(1, 0, 0, mid))],
        (1, 1): [(0, pair(0, 1, 1, HALF + mid - 1)), (1, pair(1, 1, 1, HALF + mid))],
        (1, 0): [(None, pair(0, 1, 0, HALF - 1))],
        (0, 1): [(None, pair(1, 0, 1, HALF))],
    }

    def scores(block, head):
        total = None
        for d, (qs, ks) in terms[block]:
            lo = 0 if head == 0 else width
            picked = jnp.where(heads[head], qs, 0.0)[:, lo : lo + width].astype(BF16)
            part = dot(picked, ks[:, lo : lo + width], (1, 1))
            if d is not None:
                part = jnp.where(row >= col if d == 0 else row <= col, part, 0.0)
            total = part if total is None else total + part
        return total

    for head in range(3):
        full = jnp.concatenate(
            [
                jnp.concatenate([scores((0, 0), head), scores((0, 1), head)], axis=1),
                jnp.concatenate([scores((1, 0), head), scores((1, 1), head)], axis=1),
            ],
            axis=0,
        ).astype(BF16)
        at = slice(head * width, (head + 1) * width)
        o_ref[:, at] = dot(full, v[:, at])


def pick_column(block, d, member):
    width = block.shape[1]
    per = width // SLICE
    rows = block.astype(F32)
    wide = rows[4 * d : 4 * d + 1] + rows[4 * d + 1 : 4 * d + 2]
    slim = rows[4 * d + 2 : 4 * d + 3] + rows[4 * d + 3 : 4 * d + 4]
    row = jnp.where(member >= per, slim, wide)
    want = iota((SLICE, width), 0) + SLICE * (member % per)
    hit = iota((SLICE, width), 1) == want
    return jnp.sum(jnp.where(hit, row, 0.0), axis=1, keepdims=True)


def group_kernel(place, got, pre_ref, dec_ref, tot_ref):
    member = place[1]
    count, _, width = got.shape
    summed = jnp.zeros((16, width), F32)
    for i in range(count):
        summed = summed + got[i, 2 * SLICE :, :].astype(F32)
    for d in range(2):
        at = slice(d * SLICE, (d + 1) * SLICE)
        state = jnp.zeros((SLICE, width), F32)
        total = jnp.zeros((SLICE, 1), F32)
        for i in range(count) if d == 0 else reversed(range(count)):
            pre_ref[i, at, :] = state
            dec_ref[i, at, :] = jnp.broadcast_to(jnp.exp(total), (SLICE, width))
            column = pick_column(got[i, 2 * SLICE :, :], d, member)
            state = jnp.exp(column) * state + got[i, at, :].astype(F32)
            total = total + column
        tot_ref[at, :] = state.astype(BF16)
    rows = [summed[2 * n : 2 * n + 1] + summed[2 * n + 1 : 2 * n + 2] for n in range(4)]
    tot_ref[2 * SLICE :, :] = decay_rows(rows)


def carry_kernel(place, r1, r2, r3, pre, dec, out):
    group, member, groups = place[0], place[1], place[2]
    count, _, width = pre.shape
    came = {1: r1, 2: r2, 3: r3}
    for d in range(2):
        at = slice(d * SLICE, (d + 1) * SLICE)
        carry = jnp.zeros((SLICE, width), F32)
        for back in (3, 2, 1):
            ref = came[back] if d == 0 else came[4 - back]
            live = group - back >= 0 if d == 0 else group + back < groups
            column = pick_column(ref[2 * SLICE :, :], d, member)
            moved = jnp.exp(column) * carry + ref[at, :].astype(F32)
            carry = jnp.where(live, moved, carry)
        for i in range(count):
            out[i, at, :] = (pre[i, at, :] + dec[i, at, :] * carry).astype(BF16)


def mix_kernel(states, o_ref, qf, qb, gate, gain, proj, out):
    n, width = o_ref.shape[0], states.shape[2]
    members = states.shape[0]
    entering = [
        jnp.concatenate(
            [states[j, d * SLICE : (d + 1) * SLICE, :] for j in range(members)], axis=0
        )
        for d in range(2)
    ]
    low = iota((n, width), 1) < width // 2
    mixed = []
    for head in range(3):
        at = slice(head * width, (head + 1) * width)
        total = o_ref[:, at]
        for d, q in enumerate((qf, qb)):
            if head == 0:
                total = total + dot(q[:, :width], entering[d][:width])
            else:
                keep = low if head == 1 else jnp.logical_not(low)
                own = jnp.where(keep, q[:, width:].astype(F32), 0.0).astype(BF16)
                total = total + dot(own, entering[d][width:])
        total = total * lax.rsqrt(jnp.mean(total * total, axis=1, keepdims=True) + EPS)
        total = total * gain[:, at] * jax.nn.silu(gate[:, at].astype(F32))
        mixed.append(total.astype(BF16))
    out[...] = dot(jnp.concatenate(mixed, axis=1), proj[...]).astype(BF16)


def slot_matrix(routes):
    rows = routes.shape[1]
    slots = 32 * CAP
    expert = iota((slots, rows), 0) // CAP
    first = routes[0:1] == expert
    second = routes[1:2] == expert
    named = jnp.logical_or(first, second)
    before = (iota((rows, rows), 0) < iota((rows, rows), 1)).astype(F32).astype(BF16)
    rank = dot(named.astype(F32).astype(BF16), before)
    placed = rank.astype(jnp.int32) == iota((slots, rows), 0) % CAP
    return jnp.logical_and(first, placed), jnp.logical_and(second, placed)


def dispatch_kernel(parts, skip, gain, routes, hidden_ref, out):
    mixing = parts[0].astype(F32)
    for k in range(1, parts.shape[0]):
        mixing = mixing + parts[k].astype(F32)
    hidden_bf = (skip[...].astype(F32) + mixing).astype(BF16)
    hidden_ref[...] = hidden_bf
    hidden = hidden_bf.astype(F32)
    normed = hidden * lax.rsqrt(jnp.mean(hidden * hidden, axis=1, keepdims=True) + EPS)
    normed = (normed * gain[...]).astype(BF16)
    first, second = slot_matrix(routes[...])
    chosen = jnp.logical_or(first, second).astype(F32).astype(BF16)
    out[...] = block_of(dot(chosen, normed).astype(BF16))


def rows_of(block):
    return block.astype(F32).reshape(-1, block.shape[-1]).astype(BF16)


def block_of(rows):
    return rows.astype(F32).reshape(-1, CAP, rows.shape[-1]).astype(BF16)


def split_kernel(got, low, high):
    half = got.shape[0] // 2
    low[...] = rows_of(got[:half])
    high[...] = rows_of(got[half:])


def own_kernel(low, high, a, b, c, part_low, part_high, wg, wu, wd, sems):
    moves = [
        pltpu.make_async_copy(src, dst, sems.at[n])
        for n, (src, dst) in enumerate(((a, wg), (b, wu), (c, wd)))
    ]
    for move in moves:
        move.start()
    rows = jnp.concatenate([low[...], high[...]], axis=0)
    moves[0].wait()
    gate = jax.nn.silu(dot(rows, wg[...]))
    moves[1].wait()
    act = (gate * dot(rows, wu[...])).astype(BF16)
    moves[2].wait()
    part = dot(act, wd[...]).astype(BF16)
    half = low.shape[0]
    part_low[...] = part[:half]
    part_high[...] = part[half:]


def piece_kernel(x, wg, wu, wd, out):
    rows = x[...]
    act = (jax.nn.silu(dot(rows, wg[...])) * dot(rows, wu[...])).astype(BF16)
    out[...] = dot(act, wd[...]).astype(BF16)


def add_kernel(a, b, out):
    out[...] = (a[...].astype(F32) + b[...].astype(F32)).astype(BF16)


def sum_kernel(low_a, low_b, low_c, high_a, high_b, high_c, out):
    half = out.shape[0] // 2
    f = lambda ref: ref[...].astype(F32)
    out[:half] = block_of((f(low_a) + f(low_b) + f(low_c)).astype(BF16))
    out[half:] = block_of((f(high_a) + f(high_b) + f(high_c)).astype(BF16))


def combine_kernel(hidden, back, routes, share, out):
    first, second = slot_matrix(routes[...])
    weight = jnp.where(first, share[0:1], 0.0) + jnp.where(second, share[1:2], 0.0)
    hi, lo = split_parts(weight)
    rows = rows_of(back[...])
    mixture = dot(hi, rows, (0, 0)) + dot(lo, rows, (0, 0))
    out[...] = (hidden[...].astype(F32) + mixture).astype(BF16)


def sds(shape, dtype):
    return jax.ShapeDtypeStruct(shape, dtype)


def near(shape, dtype):
    return pltpu.VMEM(shape, dtype)


def nearby(*arrays):
    return tuple(pltpu.with_memory_space_constraint(a, pltpu.VMEM) for a in arrays)


def params(mib=24):
    return pltpu.CompilerParams(vmem_limit_bytes=mib << 20)


def distant(*arrays):
    return tuple(pltpu.with_memory_space_constraint(a, pltpu.HBM) for a in arrays)


VMEM = pl.BlockSpec(memory_space=pltpu.VMEM)
SMEM = pl.BlockSpec(memory_space=pltpu.SMEM)


def cost(flops):
    return pl.CostEstimate(flops=flops, bytes_accessed=1 << 20, transcendentals=0)


def local(
    skip_stream,
    wide_probe_logits,
    narrow_probe_logits,
    wide_decay_logits,
    narrow_decay_logits,
    wide_floor_complement,
    narrow_floor_complement,
    payloads,
    result_switch_logits,
    spike_decays,
    channel_scale_vector,
    result_mapping_matrix,
    specialist_scale_vector,
    assignments,
    assignment_share,
    specialist_switch_matrix,
    specialist_raising_matrix,
    specialist_lowering_matrix,
):
    tokens, width = wide_probe_logits.shape
    rows, model = skip_stream.shape
    joint = payloads.shape[1]
    members = lax.axis_size(ZG)
    groups = lax.axis_size("zh")
    shards = lax.axis_size("tp")
    experts = lax.axis_size(SP)
    place = jnp.stack(
        [lax.axis_index("zh"), lax.axis_index(ZG), jnp.int32(groups)]
    ).astype(jnp.int32)
    decay_args = (
        wide_decay_logits,
        narrow_decay_logits,
        wide_floor_complement,
        narrow_floor_complement,
        payloads,
        spike_decays.T,
    )

    summary = pl.pallas_call(
        summary_kernel,
        out_shape=near((members, PAY, width), BF16),
        compiler_params=params(),
        cost_estimate=cost(4 << 20),
    )(*distant(*decay_args))
    by_slice = lax.all_to_all(summary, ZG, 0, 0, tiled=True)
    inside, q_fwd, q_bwd = pl.pallas_call(
        local_kernel,
        out_shape=[
            near((tokens, joint), F32),
            near((tokens, 2 * width), BF16),
            near((tokens, 2 * width), BF16),
        ],
        compiler_params=params(),
        cost_estimate=cost(64 << 20),
    )(*distant(wide_probe_logits, narrow_probe_logits, *decay_args))
    before, decayed, total = pl.pallas_call(
        group_kernel,
        in_specs=[SMEM, VMEM],
        out_shape=[
            near((members, 2 * SLICE, width), F32),
            near((members, 2 * SLICE, width), F32),
            near((PAY, width), BF16),
        ],
        compiler_params=params(),
        cost_estimate=cost(4 << 20),
    )(place, *nearby(by_slice))
    came = [
        lax.ppermute(total, "zh", [(i, (i + k) % groups) for i in range(groups)])
        for k in (1, 2, 3)
    ]
    carried = pl.pallas_call(
        carry_kernel,
        in_specs=[SMEM] + [VMEM] * 5,
        out_shape=near((members, 2 * SLICE, width), BF16),
        compiler_params=params(),
        cost_estimate=cost(4 << 20),
    )(place, *nearby(*came, before, decayed))
    entering = lax.all_to_all(carried, ZG, 0, 0, tiled=True)
    mixed = pl.pallas_call(
        mix_kernel,
        out_shape=near((tokens, model), BF16),
        compiler_params=params(),
        cost_estimate=cost(256 << 20),
    )(
        *nearby(entering, inside, q_fwd, q_bwd),
        *distant(
            result_switch_logits, channel_scale_vector.reshape(1, joint), result_mapping_matrix
        ),
    )
    parts = lax.all_to_all(mixed.reshape(shards, rows, model), "tp", 0, 0, tiled=True)
    routes = assignments.T
    share = assignment_share.T
    slots = experts * CAP
    hidden, outgoing = pl.pallas_call(
        dispatch_kernel,
        out_shape=[sds((rows, model), BF16), near((experts, CAP, model), BF16)],
        compiler_params=params(),
        cost_estimate=cost(16 << 20),
    )(*nearby(parts), *distant(skip_stream, specialist_scale_vector.reshape(1, model), routes))
    own = lax.all_to_all(outgoing, SP, 0, 0, tiled=True)

    up_ring = [(i, (i + 1) % shards) for i in range(shards)]
    down_ring = [(i, (i - 1) % shards) for i in range(shards)]

    def up(x):
        return lax.ppermute(x, "tp", up_ring)

    def down(x):
        return lax.ppermute(x, "tp", down_ring)

    half = slots // 2
    piece = near((half, model), BF16)

    def call(kernel, flops, *arrays, **rest):
        rest = {"out_shape": piece, **rest}
        return pl.pallas_call(
            kernel, compiler_params=params(), cost_estimate=cost(flops), **rest
        )(*arrays)

    weights = (
        specialist_switch_matrix[0],
        specialist_raising_matrix[0],
        specialist_lowering_matrix[0],
    )
    own_low, own_high = call(split_kernel, 1 << 20, *nearby(own), out_shape=[piece] * 2)
    left_low, right_high = up(own_low), down(own_high)
    left_high, right_low = up(own_high), down(own_low)
    sum_low, sum_high, *weights = call(
        own_kernel,
        2 << 30,
        *nearby(own_low, own_high),
        *distant(*weights),
        in_specs=[VMEM] * 2 + [pl.BlockSpec(memory_space=pl.ANY)] * 3,
        out_shape=[piece] * 2 + [near(w.shape, w.dtype) for w in weights],
        scratch_shapes=[pltpu.SemaphoreType.DMA((3,))],
    )

    def part(x):
        return call(piece_kernel, 1 << 30, *nearby(x, *weights))

    def add(a, b):
        return call(add_kernel, 1 << 20, *nearby(a, b))

    far_low, far_high = up(left_low), down(right_high)
    for_left_low, for_right_high = part(left_low), part(right_high)
    got_high, got_low = up(for_right_high), down(for_left_low)
    for_left_high, for_right_low = part(left_high), part(right_low)
    add_low = up(part(far_low))
    add_high = down(part(far_high))
    last_low = up(add(for_right_low, add_low))
    last_high = down(add(for_left_high, add_high))
    summed = call(
        sum_kernel,
        1 << 20,
        *nearby(sum_low, last_low, got_low, sum_high, last_high, got_high),
        out_shape=near((experts, CAP, model), BF16),
    )
    back = lax.all_to_all(summed, SP, 0, 0, tiled=True)
    return pl.pallas_call(
        combine_kernel,
        out_shape=sds((rows, model), BF16),
        compiler_params=params(),
        cost_estimate=cost(16 << 20),
    )(*distant(hidden), *nearby(back), *distant(routes, share))


def solution(mesh):
    torus = Mesh(
        mesh.devices.reshape(mesh.shape["grp"], 4, 4, 2, mesh.shape["tp"]),
        GRP_SP_TP,
    )
    placed = (
        P(GRP_SP_TP, None),
        P(GRP_SP, "tp"),
        P(GRP_SP, "tp"),
        P(GRP_SP, "tp"),
        P(GRP_SP, "tp"),
        P(None, "tp"),
        P(None, "tp"),
        P(GRP_SP, "tp"),
        P(GRP_SP, "tp"),
        P(GRP_SP, "tp"),
        P("tp"),
        P("tp", None),
        P(),
        P(GRP_SP_TP, None),
        P(GRP_SP_TP, None),
        P(SP, None, "tp"),
        P(SP, None, "tp"),
        P(SP, "tp", None),
    )
    return jax.shard_map(
        local, mesh=torus, in_specs=placed, out_specs=P(GRP_SP_TP, None), check_vma=False
    )
```

```python
import jax
import jax.numpy as jnp
from jax import lax
from jax.experimental import pallas as pl
from jax.experimental.pallas import tpu as pltpu
from jax.sharding import Mesh
from jax.sharding import PartitionSpec as P

F32 = jnp.float32
BF16 = jnp.bfloat16
EPS = 1e-06
HALF = 64
SLICE = 32
PAY = 80
CAP = 4
ZG = ("zl", "c")
SP = ("zh", "zl", "c")
GRP_SP = ("grp", "zh", "zl", "c")
GRP_SP_TP = ("grp", "zh", "zl", "c", "tp")


def dot(a, b, contract=(1, 0), precision=None):
    dims = (((contract[0],), (contract[1],)), ((), ()))
    return lax.dot_general(a, b, dims, precision=precision, preferred_element_type=F32)


def iota(shape, axis):
    return lax.broadcasted_iota(jnp.int32, shape, axis)


def split_parts(x):
    hi = x.astype(BF16)
    return hi, (x - hi.astype(F32)).astype(BF16)


def exact_sums(ones, x):
    hi, rest = x.astype(BF16), x
    parts = [hi]
    for _ in range(2):
        rest = rest - parts[-1].astype(F32)
        parts.append(rest.astype(BF16))
    bits = ones.astype(F32).astype(BF16)
    return dot(jnp.concatenate([bits] * 3, axis=1), jnp.concatenate(parts, axis=0))


def key_and_decay(logits, leaks, spikes):
    gate = jax.nn.sigmoid(-logits.astype(F32))
    rows = [leaks[d : d + 1] * gate for d in range(2)]
    return rows, [jnp.log1p(-k) + spikes for k in rows]


def scan_terms(wd, nd, wleak, nleak, spk):
    n, width = wd.shape
    heads = spk.shape[0]
    lane = iota((heads, 2 * width), 1)
    owner = jnp.where(lane < width, 0, jnp.where(lane < 3 * width // 2, 1, 2))
    exact = lax.Precision.HIGHEST
    spikes = dot(spk, (iota((heads, 2 * width), 0) == owner).astype(F32), (0, 0), exact)
    kw, aw = key_and_decay(wd, wleak, spikes[:, :width])
    kn, an = key_and_decay(nd, nleak, spikes[:, width:])
    row, col = iota((n, n), 0), iota((n, n), 1)
    fwd = exact_sums(row >= col, jnp.concatenate([aw[0], an[0]], axis=1))
    bwd = exact_sums(row <= col, jnp.concatenate([aw[1], an[1]], axis=1))
    keys = [jnp.concatenate([kw[d], kn[d]], axis=1) for d in range(2)]
    return keys, (fwd, bwd)


def decay_rows(rows):
    width = rows[0].shape[1]
    at = iota((16, width), 0)
    block = jnp.zeros((16, width), F32)
    for n, row in enumerate(rows):
        hi = row.astype(BF16).astype(F32)
        block = jnp.where(at == 2 * n, hi, block)
        block = jnp.where(at == 2 * n + 1, row - hi, block)
    return block.astype(BF16)


def summary_kernel(wd, nd, wleak, nleak, v, spk, out):
    keys, running = scan_terms(wd[...], nd[...], wleak[...], nleak[...], spk[...])
    n, width = wd.shape
    values = v[...]
    last = (n - 1, 0)
    rows = []
    for d in range(2):
        closing = running[d][last[d] : last[d] + 1]
        fresh = (keys[d] * jnp.exp(closing - running[d])).astype(BF16)
        wide = dot(fresh[:, :width], values[:, :width], (0, 0))
        both = dot(fresh[:, width:], values[:, width:], (0, 0))
        slim = jnp.where(iota((width, width), 0) < width // 2, both[:, :width], both[:, width:])
        state = jnp.concatenate([wide, slim], axis=0).astype(BF16)
        for j in range(out.shape[0]):
            out[j, d * SLICE : (d + 1) * SLICE, :] = state[j * SLICE : (j + 1) * SLICE]
        rows += [closing[:, :width], closing[:, width:]]
    block = decay_rows(rows)
    for j in range(out.shape[0]):
        out[j, 2 * SLICE :, :] = block


def local_kernel(wp, np_, wd, nd, wleak, nleak, v, spk, o_ref, qf_ref, qb_ref):
    keys, running = scan_terms(wd[...], nd[...], wleak[...], nleak[...], spk[...])
    _, width = wd.shape
    q = jnp.concatenate(
        [
            jax.nn.silu(wp[...].astype(F32)) * width ** (-0.5),
            jax.nn.silu(np_[...].astype(F32)) * (width // 2) ** (-0.5),
        ],
        axis=1,
    )
    qf_ref[...] = (q * jnp.exp(running[0])).astype(BF16)
    qb_ref[...] = (q * jnp.exp(running[1])).astype(BF16)
    lane = iota((HALF, 2 * width), 1)
    heads = (lane < width, (lane >= width) & (lane < 3 * width // 2), lane >= 3 * width // 2)
    row, col = iota((HALF, HALF), 0), iota((HALF, HALF), 1)

    def pair(d, t, s, ref):
        rt = running[d][t * HALF : (t + 1) * HALF]
        rs = running[d][s * HALF : (s + 1) * HALF]
        base = running[d][ref : ref + 1]
        qs = q[t * HALF : (t + 1) * HALF] * jnp.exp(rt - base)
        ks = (keys[d][s * HALF : (s + 1) * HALF] * jnp.exp(base - rs)).astype(BF16)
        return qs, ks

    mid = HALF // 2
    terms = {
        (0, 0): [(0, pair(0, 0, 0, mid - 1)), (1, pair(1, 0, 0, mid))],
        (1, 1): [(0, pair(0, 1, 1, HALF + mid - 1)), (1, pair(1, 1, 1, HALF + mid))],
        (1, 0): [(None, pair(0, 1, 0, HALF - 1))],
        (0, 1): [(None, pair(1, 0, 1, HALF))],
    }

    def scores(block, head):
        total = None
        for d, (qs, ks) in terms[block]:
            lo = 0 if head == 0 else width
            picked = jnp.where(heads[head], qs, 0.0)[:, lo : lo + width].astype(BF16)
            part = dot(picked, ks[:, lo : lo + width], (1, 1))
            if d is not None:
                part = jnp.where(row >= col if d == 0 else row <= col, part, 0.0)
            total = part if total is None else total + part
        return total

    for head in range(3):
        full = jnp.concatenate(
            [
                jnp.concatenate([scores((0, 0), head), scores((0, 1), head)], axis=1),
                jnp.concatenate([scores((1, 0), head), scores((1, 1), head)], axis=1),
            ],
            axis=0,
        ).astype(BF16)
        at = slice(head * width, (head + 1) * width)
        o_ref[:, at] = dot(full, v[:, at])


def pick_column(block, d, member):
    width = block.shape[1]
    per = width // SLICE
    rows = block.astype(F32)
    wide = rows[4 * d : 4 * d + 1] + rows[4 * d + 1 : 4 * d + 2]
    slim = rows[4 * d + 2 : 4 * d + 3] + rows[4 * d + 3 : 4 * d + 4]
    row = jnp.where(member >= per, slim, wide)
    want = iota((SLICE, width), 0) + SLICE * (member % per)
    hit = iota((SLICE, width), 1) == want
    return jnp.sum(jnp.where(hit, row, 0.0), axis=1, keepdims=True)


def group_kernel(place, got, pre_ref, dec_ref, tot_ref):
    member = place[1]
    count, _, width = got.shape
    summed = jnp.zeros((16, width), F32)
    for i in range(count):
        summed = summed + got[i, 2 * SLICE :, :].astype(F32)
    for d in range(2):
        at = slice(d * SLICE, (d + 1) * SLICE)
        state = jnp.zeros((SLICE, width), F32)
        total = jnp.zeros((SLICE, 1), F32)
        for i in range(count) if d == 0 else reversed(range(count)):
            pre_ref[i, at, :] = state
            dec_ref[i, at, :] = jnp.broadcast_to(jnp.exp(total), (SLICE, width))
            column = pick_column(got[i, 2 * SLICE :, :], d, member)
            state = jnp.exp(column) * state + got[i, at, :].astype(F32)
            total = total + column
        tot_ref[at, :] = state.astype(BF16)
    rows = [summed[2 * n : 2 * n + 1] + summed[2 * n + 1 : 2 * n + 2] for n in range(4)]
    tot_ref[2 * SLICE :, :] = decay_rows(rows)


def carry_kernel(place, r1, r2, r3, pre, dec, out):
    group, member, groups = place[0], place[1], place[2]
    count, _, width = pre.shape
    came = {1: r1, 2: r2, 3: r3}
    for d in range(2):
        at = slice(d * SLICE, (d + 1) * SLICE)
        carry = jnp.zeros((SLICE, width), F32)
        for back in (3, 2, 1):
            ref = came[back] if d == 0 else came[4 - back]
            live = group - back >= 0 if d == 0 else group + back < groups
            column = pick_column(ref[2 * SLICE :, :], d, member)
            moved = jnp.exp(column) * carry + ref[at, :].astype(F32)
            carry = jnp.where(live, moved, carry)
        for i in range(count):
            out[i, at, :] = (pre[i, at, :] + dec[i, at, :] * carry).astype(BF16)


def mix_kernel(states, o_ref, qf, qb, gate, gain, proj_far, out, proj, sem):
    fetch = pltpu.make_async_copy(proj_far, proj, sem)
    fetch.start()
    n, width = o_ref.shape[0], states.shape[2]
    members = states.shape[0]
    entering = [
        jnp.concatenate(
            [states[j, d * SLICE : (d + 1) * SLICE, :] for j in range(members)], axis=0
        )
        for d in range(2)
    ]
    low = iota((n, width), 1) < width // 2
    mixed = []
    for head in range(3):
        at = slice(head * width, (head + 1) * width)
        total = o_ref[:, at]
        for d, q in enumerate((qf, qb)):
            if head == 0:
                total = total + dot(q[:, :width], entering[d][:width])
            else:
                keep = low if head == 1 else jnp.logical_not(low)
                own = jnp.where(keep, q[:, width:].astype(F32), 0.0).astype(BF16)
                total = total + dot(own, entering[d][width:])
        total = total * lax.rsqrt(jnp.mean(total * total, axis=1, keepdims=True) + EPS)
        total = total * gain[:, at] * jax.nn.silu(gate[:, at].astype(F32))
        mixed.append(total.astype(BF16))
    fetch.wait()
    out[...] = dot(jnp.concatenate(mixed, axis=1), proj[...]).astype(BF16)


def slot_matrix(routes):
    rows = routes.shape[1]
    slots = 32 * CAP
    expert = iota((slots, rows), 0) // CAP
    first = routes[0:1] == expert
    second = routes[1:2] == expert
    named = jnp.logical_or(first, second)
    before = (iota((rows, rows), 0) < iota((rows, rows), 1)).astype(F32).astype(BF16)
    rank = dot(named.astype(F32).astype(BF16), before)
    placed = rank.astype(jnp.int32) == iota((slots, rows), 0) % CAP
    return jnp.logical_and(first, placed), jnp.logical_and(second, placed)


def route_kernel(routes, share, chosen_ref, hi_ref, lo_ref):
    first, second = slot_matrix(routes[...])
    chosen_ref[...] = jnp.logical_or(first, second).astype(F32).astype(BF16)
    weight = jnp.where(first, share[0:1], 0.0) + jnp.where(second, share[1:2], 0.0)
    hi_ref[...], lo_ref[...] = split_parts(weight)


def dispatch_kernel(parts, skip, gain, chosen, hidden_ref, out):
    mixing = parts[0].astype(F32)
    for k in range(1, parts.shape[0]):
        mixing = mixing + parts[k].astype(F32)
    hidden_bf = (skip[...].astype(F32) + mixing).astype(BF16)
    hidden_ref[...] = hidden_bf
    hidden = hidden_bf.astype(F32)
    normed = hidden * lax.rsqrt(jnp.mean(hidden * hidden, axis=1, keepdims=True) + EPS)
    normed = (normed * gain[...]).astype(BF16)
    out[...] = block_of(dot(chosen[...], normed).astype(BF16))


def rows_of(block):
    return block.astype(F32).reshape(-1, block.shape[-1]).astype(BF16)


def block_of(rows):
    return rows.astype(F32).reshape(-1, CAP, rows.shape[-1]).astype(BF16)


def split_kernel(got, low, high):
    half = got.shape[0] // 2
    low[...] = rows_of(got[:half])
    high[...] = rows_of(got[half:])


def own_kernel(low, high, a, b, c, part_low, part_high, wg, wu, wd, sems):
    moves = [
        pltpu.make_async_copy(src, dst, sems.at[n])
        for n, (src, dst) in enumerate(((a, wg), (b, wu), (c, wd)))
    ]
    for move in moves:
        move.start()
    rows = jnp.concatenate([low[...], high[...]], axis=0)
    moves[0].wait()
    gate = jax.nn.silu(dot(rows, wg[...]))
    moves[1].wait()
    act = (gate * dot(rows, wu[...])).astype(BF16)
    moves[2].wait()
    part = dot(act, wd[...]).astype(BF16)
    half = low.shape[0]
    part_low[...] = part[:half]
    part_high[...] = part[half:]


def piece_kernel(x, y, wg, wu, wd, out_x, out_y):
    rows = jnp.concatenate([x[...], y[...]], axis=0)
    act = (jax.nn.silu(dot(rows, wg[...])) * dot(rows, wu[...])).astype(BF16)
    part = dot(act, wd[...]).astype(BF16)
    half = x.shape[0]
    out_x[...] = part[:half]
    out_y[...] = part[half:]


def add_kernel(a, b, out):
    out[...] = (a[...].astype(F32) + b[...].astype(F32)).astype(BF16)


def sum_kernel(low_a, low_b, low_c, high_a, high_b, high_c, out):
    half = out.shape[0] // 2
    f = lambda ref: ref[...].astype(F32)
    out[:half] = block_of((f(low_a) + f(low_b) + f(low_c)).astype(BF16))
    out[half:] = block_of((f(high_a) + f(high_b) + f(high_c)).astype(BF16))


def combine_kernel(hidden, back, hi, lo, out):
    rows = rows_of(back[...])
    mixture = dot(hi[...], rows, (0, 0)) + dot(lo[...], rows, (0, 0))
    out[...] = (hidden[...].astype(F32) + mixture).astype(BF16)


def sds(shape, dtype):
    return jax.ShapeDtypeStruct(shape, dtype)


def near(shape, dtype):
    return pltpu.VMEM(shape, dtype)


def nearby(*arrays):
    return tuple(pltpu.with_memory_space_constraint(a, pltpu.VMEM) for a in arrays)


def params(mib=24):
    return pltpu.CompilerParams(vmem_limit_bytes=mib << 20)


def distant(*arrays):
    return tuple(pltpu.with_memory_space_constraint(a, pltpu.HBM) for a in arrays)


VMEM = pl.BlockSpec(memory_space=pltpu.VMEM)
SMEM = pl.BlockSpec(memory_space=pltpu.SMEM)


def cost(flops):
    return pl.CostEstimate(flops=flops, bytes_accessed=1 << 20, transcendentals=0)


def local(
    skip_stream,
    wide_probe_logits,
    narrow_probe_logits,
    wide_decay_logits,
    narrow_decay_logits,
    wide_floor_complement,
    narrow_floor_complement,
    payloads,
    result_switch_logits,
    spike_decays,
    channel_scale_vector,
    result_mapping_matrix,
    specialist_scale_vector,
    assignments,
    assignment_share,
    specialist_switch_matrix,
    specialist_raising_matrix,
    specialist_lowering_matrix,
):
    tokens, width = wide_probe_logits.shape
    rows, model = skip_stream.shape
    joint = payloads.shape[1]
    members = lax.axis_size(ZG)
    groups = lax.axis_size("zh")
    shards = lax.axis_size("tp")
    experts = lax.axis_size(SP)
    place = jnp.stack(
        [lax.axis_index("zh"), lax.axis_index(ZG), jnp.int32(groups)]
    ).astype(jnp.int32)
    decay_args = (
        wide_decay_logits,
        narrow_decay_logits,
        wide_floor_complement,
        narrow_floor_complement,
        payloads,
        spike_decays.T,
    )

    summary = pl.pallas_call(
        summary_kernel,
        out_shape=near((members, PAY, width), BF16),
        compiler_params=params(),
        cost_estimate=cost(4 << 20),
    )(*distant(*decay_args))
    by_slice = lax.all_to_all(summary, ZG, 0, 0, tiled=True)
    slots = experts * CAP
    chosen, share_hi, share_lo = pl.pallas_call(
        route_kernel,
        out_shape=[sds((slots, rows), BF16)] * 3,
        compiler_params=params(),
        cost_estimate=cost(1 << 20),
    )(*distant(assignments.T, assignment_share.T))
    inside, q_fwd, q_bwd = pl.pallas_call(
        local_kernel,
        out_shape=[
            near((tokens, joint), F32),
            near((tokens, 2 * width), BF16),
            near((tokens, 2 * width), BF16),
        ],
        compiler_params=params(),
        cost_estimate=cost(64 << 20),
    )(*distant(wide_probe_logits, narrow_probe_logits, *decay_args))
    before, decayed, total = pl.pallas_call(
        group_kernel,
        in_specs=[SMEM, VMEM],
        out_shape=[
            near((members, 2 * SLICE, width), F32),
            near((members, 2 * SLICE, width), F32),
            near((PAY, width), BF16),
        ],
        compiler_params=params(),
        cost_estimate=cost(4 << 20),
    )(place, *nearby(by_slice))
    came = [
        lax.ppermute(total, "zh", [(i, (i + k) % groups) for i in range(groups)])
        for k in (1, 2, 3)
    ]
    carried = pl.pallas_call(
        carry_kernel,
        in_specs=[SMEM] + [VMEM] * 5,
        out_shape=near((members, 2 * SLICE, width), BF16),
        compiler_params=params(),
        cost_estimate=cost(4 << 20),
    )(place, *nearby(*came, before, decayed))
    entering = lax.all_to_all(carried, ZG, 0, 0, tiled=True)
    mixed = pl.pallas_call(
        mix_kernel,
        in_specs=[VMEM] * 6 + [pl.BlockSpec(memory_space=pl.ANY)],
        out_shape=near((tokens, model), BF16),
        scratch_shapes=[
            pltpu.VMEM(result_mapping_matrix.shape, BF16),
            pltpu.SemaphoreType.DMA,
        ],
        compiler_params=params(),
        cost_estimate=cost(256 << 20),
    )(
        *nearby(entering, inside, q_fwd, q_bwd),
        *distant(
            result_switch_logits, channel_scale_vector.reshape(1, joint), result_mapping_matrix
        ),
    )
    parts = lax.all_to_all(mixed.reshape(shards, rows, model), "tp", 0, 0, tiled=True)
    hidden, outgoing = pl.pallas_call(
        dispatch_kernel,
        out_shape=[sds((rows, model), BF16), near((experts, CAP, model), BF16)],
        compiler_params=params(),
        cost_estimate=cost(16 << 20),
    )(*nearby(parts), *distant(skip_stream, specialist_scale_vector.reshape(1, model), chosen))
    own = lax.all_to_all(outgoing, SP, 0, 0, tiled=True)

    up_ring = [(i, (i + 1) % shards) for i in range(shards)]
    down_ring = [(i, (i - 1) % shards) for i in range(shards)]

    def up(x):
        return lax.ppermute(x, "tp", up_ring)

    def down(x):
        return lax.ppermute(x, "tp", down_ring)

    half = slots // 2
    piece = near((half, model), BF16)

    def call(kernel, flops, *arrays, **rest):
        rest = {"out_shape": piece, **rest}
        return pl.pallas_call(
            kernel, compiler_params=params(), cost_estimate=cost(flops), **rest
        )(*arrays)

    weights = (
        specialist_switch_matrix[0],
        specialist_raising_matrix[0],
        specialist_lowering_matrix[0],
    )
    own_low, own_high = call(split_kernel, 1 << 20, *nearby(own), out_shape=[piece] * 2)
    left_low, right_high = up(own_low), down(own_high)
    left_high, right_low = up(own_high), down(own_low)
    sum_low, sum_high, *weights = call(
        own_kernel,
        2 << 30,
        *nearby(own_low, own_high),
        *distant(*weights),
        in_specs=[VMEM] * 2 + [pl.BlockSpec(memory_space=pl.ANY)] * 3,
        out_shape=[piece] * 2 + [near(w.shape, w.dtype) for w in weights],
        scratch_shapes=[pltpu.SemaphoreType.DMA((3,))],
    )

    def part(x, y):
        return call(piece_kernel, 2 << 30, *nearby(x, y, *weights), out_shape=[piece] * 2)

    def add(a, b):
        return call(add_kernel, 1 << 20, *nearby(a, b))

    far_low, far_high = up(left_low), down(right_high)
    for_left_low, for_right_high = part(left_low, right_high)
    got_high, got_low = up(for_right_high), down(for_left_low)
    for_left_high, for_right_low = part(left_high, right_low)
    for_far_low, for_far_high = part(far_low, far_high)
    add_low, add_high = up(for_far_low), down(for_far_high)
    last_low = up(add(for_right_low, add_low))
    last_high = down(add(for_left_high, add_high))
    summed = call(
        sum_kernel,
        1 << 20,
        *nearby(sum_low, last_low, got_low, sum_high, last_high, got_high),
        out_shape=near((experts, CAP, model), BF16),
    )
    back = lax.all_to_all(summed, SP, 0, 0, tiled=True)
    return pl.pallas_call(
        combine_kernel,
        out_shape=sds((rows, model), BF16),
        compiler_params=params(),
        cost_estimate=cost(16 << 20),
    )(*distant(hidden), *nearby(back), *distant(share_hi, share_lo))


def solution(mesh):
    torus = Mesh(
        mesh.devices.reshape(mesh.shape["grp"], 4, 4, 2, mesh.shape["tp"]),
        GRP_SP_TP,
    )
    placed = (
        P(GRP_SP_TP, None),
        P(GRP_SP, "tp"),
        P(GRP_SP, "tp"),
        P(GRP_SP, "tp"),
        P(GRP_SP, "tp"),
        P(None, "tp"),
        P(None, "tp"),
        P(GRP_SP, "tp"),
        P(GRP_SP, "tp"),
        P(GRP_SP, "tp"),
        P("tp"),
        P("tp", None),
        P(),
        P(GRP_SP_TP, None),
        P(GRP_SP_TP, None),
        P(SP, None, "tp"),
        P(SP, None, "tp"),
        P(SP, "tp", None),
    )
    return jax.shard_map(
        local, mesh=torus, in_specs=placed, out_specs=P(GRP_SP_TP, None), check_vma=False
    )
```

```python
import jax
import jax.numpy as jnp
from jax import lax
from jax.experimental import pallas as pl
from jax.experimental.pallas import tpu as pltpu
from jax.sharding import Mesh
from jax.sharding import PartitionSpec as P

F32 = jnp.float32
BF16 = jnp.bfloat16
EPS = 1e-06
HALF = 64
SLICE = 32
PAY = 80
CAP = 4
ZG = ("zl", "c")
SP = ("zh", "zl", "c")
GRP_SP = ("grp", "zh", "zl", "c")
GRP_SP_TP = ("grp", "zh", "zl", "c", "tp")


def dot(a, b, contract=(1, 0), precision=None):
    dims = (((contract[0],), (contract[1],)), ((), ()))
    return lax.dot_general(a, b, dims, precision=precision, preferred_element_type=F32)


def iota(shape, axis):
    return lax.broadcasted_iota(jnp.int32, shape, axis)


def split_parts(x):
    hi = x.astype(BF16)
    return hi, (x - hi.astype(F32)).astype(BF16)


def exact_sums(ones, x):
    hi, rest = x.astype(BF16), x
    parts = [hi]
    for _ in range(2):
        rest = rest - parts[-1].astype(F32)
        parts.append(rest.astype(BF16))
    bits = ones.astype(F32).astype(BF16)
    return dot(jnp.concatenate([bits] * 3, axis=1), jnp.concatenate(parts, axis=0))


def key_and_decay(logits, leaks, spikes):
    gate = jax.nn.sigmoid(-logits.astype(F32))
    rows = [leaks[d : d + 1] * gate for d in range(2)]
    return rows, [jnp.log1p(-k) + spikes for k in rows]


def scan_terms(wd, nd, wleak, nleak, spk):
    n, width = wd.shape
    heads = spk.shape[0]
    lane = iota((heads, 2 * width), 1)
    owner = jnp.where(lane < width, 0, jnp.where(lane < 3 * width // 2, 1, 2))
    exact = lax.Precision.HIGHEST
    spikes = dot(spk, (iota((heads, 2 * width), 0) == owner).astype(F32), (0, 0), exact)
    kw, aw = key_and_decay(wd, wleak, spikes[:, :width])
    kn, an = key_and_decay(nd, nleak, spikes[:, width:])
    row, col = iota((n, n), 0), iota((n, n), 1)
    fwd = exact_sums(row >= col, jnp.concatenate([aw[0], an[0]], axis=1))
    bwd = exact_sums(row <= col, jnp.concatenate([aw[1], an[1]], axis=1))
    keys = [jnp.concatenate([kw[d], kn[d]], axis=1) for d in range(2)]
    return keys, (fwd, bwd)


def decay_rows(rows):
    width = rows[0].shape[1]
    at = iota((16, width), 0)
    block = jnp.zeros((16, width), F32)
    for n, row in enumerate(rows):
        hi = row.astype(BF16).astype(F32)
        block = jnp.where(at == 2 * n, hi, block)
        block = jnp.where(at == 2 * n + 1, row - hi, block)
    return block.astype(BF16)


def summary_kernel(wd, nd, wleak, nleak, v, spk, out):
    keys, running = scan_terms(wd[...], nd[...], wleak[...], nleak[...], spk[...])
    n, width = wd.shape
    values = v[...]
    last = (n - 1, 0)
    rows = []
    for d in range(2):
        closing = running[d][last[d] : last[d] + 1]
        fresh = (keys[d] * jnp.exp(closing - running[d])).astype(BF16)
        wide = dot(fresh[:, :width], values[:, :width], (0, 0))
        both = dot(fresh[:, width:], values[:, width:], (0, 0))
        slim = jnp.where(iota((width, width), 0) < width // 2, both[:, :width], both[:, width:])
        state = jnp.concatenate([wide, slim], axis=0).astype(BF16)
        for j in range(out.shape[0]):
            out[j, d * SLICE : (d + 1) * SLICE, :] = state[j * SLICE : (j + 1) * SLICE]
        rows += [closing[:, :width], closing[:, width:]]
    block = decay_rows(rows)
    for j in range(out.shape[0]):
        out[j, 2 * SLICE :, :] = block


def local_kernel(
    wp, np_, wd, nd, wleak, nleak, v, spk, gate, gain, proj_far, o_ref, qf_ref, qb_ref, scale_ref, proj, sem
):
    fetch = pltpu.make_async_copy(proj_far, proj, sem)
    fetch.start()
    scale_ref[...] = gain[...] * jax.nn.silu(gate[...].astype(F32))
    keys, running = scan_terms(wd[...], nd[...], wleak[...], nleak[...], spk[...])
    _, width = wd.shape
    q = jnp.concatenate(
        [
            jax.nn.silu(wp[...].astype(F32)) * width ** (-0.5),
            jax.nn.silu(np_[...].astype(F32)) * (width // 2) ** (-0.5),
        ],
        axis=1,
    )
    qf_ref[...] = (q * jnp.exp(running[0])).astype(BF16)
    qb_ref[...] = (q * jnp.exp(running[1])).astype(BF16)
    lane = iota((HALF, 2 * width), 1)
    heads = (lane < width, (lane >= width) & (lane < 3 * width // 2), lane >= 3 * width // 2)
    row, col = iota((HALF, HALF), 0), iota((HALF, HALF), 1)

    def pair(d, t, s, ref):
        rt = running[d][t * HALF : (t + 1) * HALF]
        rs = running[d][s * HALF : (s + 1) * HALF]
        base = running[d][ref : ref + 1]
        qs = q[t * HALF : (t + 1) * HALF] * jnp.exp(rt - base)
        ks = (keys[d][s * HALF : (s + 1) * HALF] * jnp.exp(base - rs)).astype(BF16)
        return qs, ks

    mid = HALF // 2
    terms = {
        (0, 0): [(0, pair(0, 0, 0, mid - 1)), (1, pair(1, 0, 0, mid))],
        (1, 1): [(0, pair(0, 1, 1, HALF + mid - 1)), (1, pair(1, 1, 1, HALF + mid))],
        (1, 0): [(None, pair(0, 1, 0, HALF - 1))],
        (0, 1): [(None, pair(1, 0, 1, HALF))],
    }

    def scores(block, head):
        total = None
        for d, (qs, ks) in terms[block]:
            lo = 0 if head == 0 else width
            picked = jnp.where(heads[head], qs, 0.0)[:, lo : lo + width].astype(BF16)
            part = dot(picked, ks[:, lo : lo + width], (1, 1))
            if d is not None:
                part = jnp.where(row >= col if d == 0 else row <= col, part, 0.0)
            total = part if total is None else total + part
        return total

    for head in range(3):
        full = jnp.concatenate(
            [
                jnp.concatenate([scores((0, 0), head), scores((0, 1), head)], axis=1),
                jnp.concatenate([scores((1, 0), head), scores((1, 1), head)], axis=1),
            ],
            axis=0,
        ).astype(BF16)
        at = slice(head * width, (head + 1) * width)
        o_ref[:, at] = dot(full, v[:, at])
    fetch.wait()


def pick_column(block, d, member):
    width = block.shape[1]
    per = width // SLICE
    rows = block.astype(F32)
    wide = rows[4 * d : 4 * d + 1] + rows[4 * d + 1 : 4 * d + 2]
    slim = rows[4 * d + 2 : 4 * d + 3] + rows[4 * d + 3 : 4 * d + 4]
    row = jnp.where(member >= per, slim, wide)
    want = iota((SLICE, width), 0) + SLICE * (member % per)
    hit = iota((SLICE, width), 1) == want
    return jnp.sum(jnp.where(hit, row, 0.0), axis=1, keepdims=True)


def group_kernel(place, got, pre_ref, dec_ref, tot_ref):
    member = place[1]
    count, _, width = got.shape
    summed = jnp.zeros((16, width), F32)
    for i in range(count):
        summed = summed + got[i, 2 * SLICE :, :].astype(F32)
    for d in range(2):
        at = slice(d * SLICE, (d + 1) * SLICE)
        state = jnp.zeros((SLICE, width), F32)
        total = jnp.zeros((SLICE, 1), F32)
        for i in range(count) if d == 0 else reversed(range(count)):
            pre_ref[i, at, :] = state
            dec_ref[i, at, :] = jnp.broadcast_to(jnp.exp(total), (SLICE, width))
            column = pick_column(got[i, 2 * SLICE :, :], d, member)
            state = jnp.exp(column) * state + got[i, at, :].astype(F32)
            total = total + column
        tot_ref[at, :] = state.astype(BF16)
    rows = [summed[2 * n : 2 * n + 1] + summed[2 * n + 1 : 2 * n + 2] for n in range(4)]
    tot_ref[2 * SLICE :, :] = decay_rows(rows)


def carry_kernel(place, r1, r2, r3, pre, dec, out):
    group, member, groups = place[0], place[1], place[2]
    count, _, width = pre.shape
    came = {1: r1, 2: r2, 3: r3}
    for d in range(2):
        at = slice(d * SLICE, (d + 1) * SLICE)
        carry = jnp.zeros((SLICE, width), F32)
        for back in (3, 2, 1):
            ref = came[back] if d == 0 else came[4 - back]
            live = group - back >= 0 if d == 0 else group + back < groups
            column = pick_column(ref[2 * SLICE :, :], d, member)
            moved = jnp.exp(column) * carry + ref[at, :].astype(F32)
            carry = jnp.where(live, moved, carry)
        for i in range(count):
            out[i, at, :] = (pre[i, at, :] + dec[i, at, :] * carry).astype(BF16)


def mix_kernel(states, o_ref, qf, qb, scale, proj, out):
    n, width = o_ref.shape[0], states.shape[2]
    members = states.shape[0]
    entering = [
        jnp.concatenate(
            [states[j, d * SLICE : (d + 1) * SLICE, :] for j in range(members)], axis=0
        )
        for d in range(2)
    ]
    low = iota((n, width), 1) < width // 2
    mixed = []
    for head in range(3):
        at = slice(head * width, (head + 1) * width)
        total = o_ref[:, at]
        for d, q in enumerate((qf, qb)):
            if head == 0:
                total = total + dot(q[:, :width], entering[d][:width])
            else:
                keep = low if head == 1 else jnp.logical_not(low)
                own = jnp.where(keep, q[:, width:].astype(F32), 0.0).astype(BF16)
                total = total + dot(own, entering[d][width:])
        total = total * lax.rsqrt(jnp.mean(total * total, axis=1, keepdims=True) + EPS)
        total = total * scale[:, at]
        mixed.append(total.astype(BF16))
    out[...] = dot(jnp.concatenate(mixed, axis=1), proj[...]).astype(BF16)


def slot_matrix(routes):
    rows = routes.shape[1]
    slots = 32 * CAP
    expert = iota((slots, rows), 0) // CAP
    first = routes[0:1] == expert
    second = routes[1:2] == expert
    named = jnp.logical_or(first, second)
    before = (iota((rows, rows), 0) < iota((rows, rows), 1)).astype(F32).astype(BF16)
    rank = dot(named.astype(F32).astype(BF16), before)
    placed = rank.astype(jnp.int32) == iota((slots, rows), 0) % CAP
    return jnp.logical_and(first, placed), jnp.logical_and(second, placed)


def route_kernel(routes, share, skip, gain, chosen_ref, hi_ref, lo_ref, skip_ref, gain_ref):
    skip_ref[...] = skip[...]
    gain_ref[...] = gain[...]
    first, second = slot_matrix(routes[...])
    chosen_ref[...] = jnp.logical_or(first, second).astype(F32).astype(BF16)
    weight = jnp.where(first, share[0:1], 0.0) + jnp.where(second, share[1:2], 0.0)
    hi_ref[...], lo_ref[...] = split_parts(weight)


def dispatch_kernel(parts, skip, gain, chosen, hidden_ref, out):
    mixing = parts[0].astype(F32)
    for k in range(1, parts.shape[0]):
        mixing = mixing + parts[k].astype(F32)
    hidden_bf = (skip[...].astype(F32) + mixing).astype(BF16)
    hidden_ref[...] = hidden_bf
    hidden = hidden_bf.astype(F32)
    normed = hidden * lax.rsqrt(jnp.mean(hidden * hidden, axis=1, keepdims=True) + EPS)
    normed = (normed * gain[...]).astype(BF16)
    out[...] = block_of(dot(chosen[...], normed).astype(BF16))


def rows_of(block):
    return block.astype(F32).reshape(-1, block.shape[-1]).astype(BF16)


def block_of(rows):
    return rows.astype(F32).reshape(-1, CAP, rows.shape[-1]).astype(BF16)


def split_kernel(got, low, high):
    half = got.shape[0] // 2
    low[...] = rows_of(got[:half])
    high[...] = rows_of(got[half:])


def own_kernel(low, high, a, b, c, part_low, part_high, wg, wu, wd, sems):
    moves = [
        pltpu.make_async_copy(src, dst, sems.at[n])
        for n, (src, dst) in enumerate(((a, wg), (b, wu), (c, wd)))
    ]
    for move in moves:
        move.start()
    rows = jnp.concatenate([low[...], high[...]], axis=0)
    moves[0].wait()
    gate = jax.nn.silu(dot(rows, wg[...]))
    moves[1].wait()
    act = (gate * dot(rows, wu[...])).astype(BF16)
    moves[2].wait()
    part = dot(act, wd[...]).astype(BF16)
    half = low.shape[0]
    part_low[...] = part[:half]
    part_high[...] = part[half:]


def piece_kernel(x, y, wg, wu, wd, out_x, out_y):
    rows = jnp.concatenate([x[...], y[...]], axis=0)
    act = (jax.nn.silu(dot(rows, wg[...])) * dot(rows, wu[...])).astype(BF16)
    part = dot(act, wd[...]).astype(BF16)
    half = x.shape[0]
    out_x[...] = part[:half]
    out_y[...] = part[half:]


def add_kernel(a, b, out):
    out[...] = (a[...].astype(F32) + b[...].astype(F32)).astype(BF16)


def sum_kernel(low_a, low_b, low_c, high_a, high_b, high_c, out):
    half = out.shape[0] // 2
    f = lambda ref: ref[...].astype(F32)
    out[:half] = block_of((f(low_a) + f(low_b) + f(low_c)).astype(BF16))
    out[half:] = block_of((f(high_a) + f(high_b) + f(high_c)).astype(BF16))


def combine_kernel(hidden, back, hi, lo, out):
    rows = rows_of(back[...])
    mixture = dot(hi[...], rows, (0, 0)) + dot(lo[...], rows, (0, 0))
    out[...] = (hidden[...].astype(F32) + mixture).astype(BF16)


def sds(shape, dtype):
    return jax.ShapeDtypeStruct(shape, dtype)


def near(shape, dtype):
    return pltpu.VMEM(shape, dtype)


def nearby(*arrays):
    return tuple(pltpu.with_memory_space_constraint(a, pltpu.VMEM) for a in arrays)


def params(mib=24):
    return pltpu.CompilerParams(vmem_limit_bytes=mib << 20)


def distant(*arrays):
    return tuple(pltpu.with_memory_space_constraint(a, pltpu.HBM) for a in arrays)


VMEM = pl.BlockSpec(memory_space=pltpu.VMEM)
SMEM = pl.BlockSpec(memory_space=pltpu.SMEM)


def cost(flops):
    return pl.CostEstimate(flops=flops, bytes_accessed=1 << 20, transcendentals=0)


def local(
    skip_stream,
    wide_probe_logits,
    narrow_probe_logits,
    wide_decay_logits,
    narrow_decay_logits,
    wide_floor_complement,
    narrow_floor_complement,
    payloads,
    result_switch_logits,
    spike_decays,
    channel_scale_vector,
    result_mapping_matrix,
    specialist_scale_vector,
    assignments,
    assignment_share,
    specialist_switch_matrix,
    specialist_raising_matrix,
    specialist_lowering_matrix,
):
    tokens, width = wide_probe_logits.shape
    rows, model = skip_stream.shape
    joint = payloads.shape[1]
    members = lax.axis_size(ZG)
    groups = lax.axis_size("zh")
    shards = lax.axis_size("tp")
    experts = lax.axis_size(SP)
    place = jnp.stack(
        [lax.axis_index("zh"), lax.axis_index(ZG), jnp.int32(groups)]
    ).astype(jnp.int32)
    decay_args = (
        wide_decay_logits,
        narrow_decay_logits,
        wide_floor_complement,
        narrow_floor_complement,
        payloads,
        spike_decays.T,
    )

    summary = pl.pallas_call(
        summary_kernel,
        out_shape=near((members, PAY, width), BF16),
        compiler_params=params(),
        cost_estimate=cost(4 << 20),
    )(*distant(*decay_args))
    by_slice = lax.all_to_all(summary, ZG, 0, 0, tiled=True)
    slots = experts * CAP
    chosen, share_hi, share_lo, skip, norm_gain = pl.pallas_call(
        route_kernel,
        out_shape=[near((slots, rows), BF16)] * 3
        + [near((rows, model), BF16), near((1, model), F32)],
        compiler_params=params(),
        cost_estimate=cost(1 << 20),
    )(
        *distant(
            assignments.T,
            assignment_share.T,
            skip_stream,
            specialist_scale_vector.reshape(1, model),
        )
    )
    inside, q_fwd, q_bwd, scale, projection = pl.pallas_call(
        local_kernel,
        in_specs=[VMEM] * 10 + [pl.BlockSpec(memory_space=pl.ANY)],
        out_shape=[
            near((tokens, joint), F32),
            near((tokens, 2 * width), BF16),
            near((tokens, 2 * width), BF16),
            near((tokens, joint), F32),
            near(result_mapping_matrix.shape, BF16),
        ],
        scratch_shapes=[pltpu.SemaphoreType.DMA],
        compiler_params=params(),
        cost_estimate=cost(64 << 20),
    )(
        *distant(
            wide_probe_logits,
            narrow_probe_logits,
            *decay_args,
            result_switch_logits,
            channel_scale_vector.reshape(1, joint),
            result_mapping_matrix,
        )
    )
    before, decayed, total = pl.pallas_call(
        group_kernel,
        in_specs=[SMEM, VMEM],
        out_shape=[
            near((members, 2 * SLICE, width), F32),
            near((members, 2 * SLICE, width), F32),
            near((PAY, width), BF16),
        ],
        compiler_params=params(),
        cost_estimate=cost(4 << 20),
    )(place, *nearby(by_slice))
    came = [
        lax.ppermute(total, "zh", [(i, (i + k) % groups) for i in range(groups)])
        for k in (1, 2, 3)
    ]
    carried = pl.pallas_call(
        carry_kernel,
        in_specs=[SMEM] + [VMEM] * 5,
        out_shape=near((members, 2 * SLICE, width), BF16),
        compiler_params=params(),
        cost_estimate=cost(4 << 20),
    )(place, *nearby(*came, before, decayed))
    entering = lax.all_to_all(carried, ZG, 0, 0, tiled=True)
    mixed = pl.pallas_call(
        mix_kernel,
        out_shape=near((tokens, model), BF16),
        compiler_params=params(),
        cost_estimate=cost(256 << 20),
    )(*nearby(entering, inside, q_fwd, q_bwd, scale, projection))
    parts = lax.all_to_all(mixed.reshape(shards, rows, model), "tp", 0, 0, tiled=True)
    hidden, outgoing = pl.pallas_call(
        dispatch_kernel,
        out_shape=[near((rows, model), BF16), near((experts, CAP, model), BF16)],
        compiler_params=params(),
        cost_estimate=cost(16 << 20),
    )(*nearby(parts, skip, norm_gain, chosen))
    own = lax.all_to_all(outgoing, SP, 0, 0, tiled=True)

    up_ring = [(i, (i + 1) % shards) for i in range(shards)]
    down_ring = [(i, (i - 1) % shards) for i in range(shards)]

    def up(x):
        return lax.ppermute(x, "tp", up_ring)

    def down(x):
        return lax.ppermute(x, "tp", down_ring)

    half = slots // 2
    piece = near((half, model), BF16)

    def call(kernel, flops, *arrays, **rest):
        rest = {"out_shape": piece, **rest}
        return pl.pallas_call(
            kernel, compiler_params=params(), cost_estimate=cost(flops), **rest
        )(*arrays)

    weights = (
        specialist_switch_matrix[0],
        specialist_raising_matrix[0],
        specialist_lowering_matrix[0],
    )
    own_low, own_high = call(split_kernel, 1 << 20, *nearby(own), out_shape=[piece] * 2)
    left_low, right_high = up(own_low), down(own_high)
    left_high, right_low = up(own_high), down(own_low)
    sum_low, sum_high, *weights = call(
        own_kernel,
        2 << 30,
        *nearby(own_low, own_high),
        *distant(*weights),
        in_specs=[VMEM] * 2 + [pl.BlockSpec(memory_space=pl.ANY)] * 3,
        out_shape=[piece] * 2 + [near(w.shape, w.dtype) for w in weights],
        scratch_shapes=[pltpu.SemaphoreType.DMA((3,))],
    )

    def part(x, y):
        return call(piece_kernel, 2 << 30, *nearby(x, y, *weights), out_shape=[piece] * 2)

    def add(a, b):
        return call(add_kernel, 1 << 20, *nearby(a, b))

    far_low, far_high = up(left_low), down(right_high)
    for_left_low, for_right_high = part(left_low, right_high)
    got_high, got_low = up(for_right_high), down(for_left_low)
    for_left_high, for_right_low = part(left_high, right_low)
    for_far_low, for_far_high = part(far_low, far_high)
    add_low, add_high = up(for_far_low), down(for_far_high)
    last_low = up(add(for_right_low, add_low))
    last_high = down(add(for_left_high, add_high))
    summed = call(
        sum_kernel,
        1 << 20,
        *nearby(sum_low, last_low, got_low, sum_high, last_high, got_high),
        out_shape=near((experts, CAP, model), BF16),
    )
    back = lax.all_to_all(summed, SP, 0, 0, tiled=True)
    return pl.pallas_call(
        combine_kernel,
        out_shape=sds((rows, model), BF16),
        compiler_params=params(),
        cost_estimate=cost(16 << 20),
    )(*nearby(hidden, back, share_hi, share_lo))


def solution(mesh):
    torus = Mesh(
        mesh.devices.reshape(mesh.shape["grp"], 4, 4, 2, mesh.shape["tp"]),
        GRP_SP_TP,
    )
    placed = (
        P(GRP_SP_TP, None),
        P(GRP_SP, "tp"),
        P(GRP_SP, "tp"),
        P(GRP_SP, "tp"),
        P(GRP_SP, "tp"),
        P(None, "tp"),
        P(None, "tp"),
        P(GRP_SP, "tp"),
        P(GRP_SP, "tp"),
        P(GRP_SP, "tp"),
        P("tp"),
        P("tp", None),
        P(),
        P(GRP_SP_TP, None),
        P(GRP_SP_TP, None),
        P(SP, None, "tp"),
        P(SP, None, "tp"),
        P(SP, "tp", None),
    )
    return jax.shard_map(
        local, mesh=torus, in_specs=placed, out_specs=P(GRP_SP_TP, None), check_vma=False
    )
```

```python
import jax
import jax.numpy as jnp
from jax import lax
from jax.experimental import pallas as pl
from jax.experimental.pallas import tpu as pltpu
from jax.sharding import Mesh
from jax.sharding import PartitionSpec as P

F32 = jnp.float32
BF16 = jnp.bfloat16
EPS = 1e-06
HALF = 64
SLICE = 32
PAY = 80
CAP = 4
ZG = ("zl", "c")
SP = ("zh", "zl", "c")
GRP_SP = ("grp", "zh", "zl", "c")
GRP_SP_TP = ("grp", "zh", "zl", "c", "tp")


def dot(a, b, contract=(1, 0), precision=None):
    dims = (((contract[0],), (contract[1],)), ((), ()))
    return lax.dot_general(a, b, dims, precision=precision, preferred_element_type=F32)


def iota(shape, axis):
    return lax.broadcasted_iota(jnp.int32, shape, axis)


def split_parts(x):
    hi = x.astype(BF16)
    return hi, (x - hi.astype(F32)).astype(BF16)


def exact_sums(ones, x, side=1):
    hi, rest = x.astype(BF16), x
    parts = [hi]
    for _ in range(2):
        rest = rest - parts[-1].astype(F32)
        parts.append(rest.astype(BF16))
    bits = ones.astype(F32).astype(BF16)
    stacked = jnp.concatenate([p.astype(F32) for p in parts], axis=0).astype(BF16)
    if side == 0:
        return dot(stacked, jnp.concatenate([bits] * 3, axis=0), (0, 0))
    return dot(jnp.concatenate([bits] * 3, axis=1), stacked)


def key_and_decay(logits, leaks, spikes):
    gate = jax.nn.sigmoid(-logits.astype(F32))
    rows = [leaks[d : d + 1] * gate for d in range(2)]
    return rows, [jnp.log1p(-k) + spikes for k in rows]


def scan_terms(wd, nd, wleak, nleak, spk):
    n, width = wd.shape
    heads = spk.shape[0]
    lane = iota((heads, 2 * width), 1)
    owner = jnp.where(lane < width, 0, jnp.where(lane < 3 * width // 2, 1, 2))
    spikes = exact_sums(iota((heads, 2 * width), 0) == owner, spk, 0)
    kw, aw = key_and_decay(wd, wleak, spikes[:, :width])
    kn, an = key_and_decay(nd, nleak, spikes[:, width:])
    row, col = iota((n, n), 0), iota((n, n), 1)
    fwd = exact_sums(row >= col, jnp.concatenate([aw[0], an[0]], axis=1))
    bwd = exact_sums(row <= col, jnp.concatenate([aw[1], an[1]], axis=1))
    keys = [jnp.concatenate([kw[d], kn[d]], axis=1) for d in range(2)]
    return keys, (fwd, bwd)


def decay_rows(rows):
    width = rows[0].shape[1]
    at = iota((16, width), 0)
    block = jnp.zeros((16, width), F32)
    for n, row in enumerate(rows):
        hi = row.astype(BF16).astype(F32)
        block = jnp.where(at == 2 * n, hi, block)
        block = jnp.where(at == 2 * n + 1, row - hi, block)
    return block.astype(BF16)


def summary_kernel(wd, nd, wleak, nleak, v, spk, out):
    keys, running = scan_terms(wd[...], nd[...], wleak[...], nleak[...], spk[...])
    n, width = wd.shape
    values = v[...]
    last = (n - 1, 0)
    rows = []
    for d in range(2):
        closing = running[d][last[d] : last[d] + 1]
        fresh = (keys[d] * jnp.exp(closing - running[d])).astype(BF16)
        wide = dot(fresh[:, :width], values[:, :width], (0, 0))
        both = dot(fresh[:, width:], values[:, width:], (0, 0))
        slim = jnp.where(iota((width, width), 0) < width // 2, both[:, :width], both[:, width:])
        state = jnp.concatenate([wide, slim], axis=0).astype(BF16)
        for j in range(out.shape[0]):
            out[j, d * SLICE : (d + 1) * SLICE, :] = state[j * SLICE : (j + 1) * SLICE]
        rows += [closing[:, :width], closing[:, width:]]
    block = decay_rows(rows)
    for j in range(out.shape[0]):
        out[j, 2 * SLICE :, :] = block


def local_kernel(
    wp, np_, wd, nd, wleak, nleak, v, spk, gate, gain, proj_far, o_ref, qf_ref, qb_ref, scale_ref, proj, sem
):
    fetch = pltpu.make_async_copy(proj_far, proj, sem)
    fetch.start()
    scale_ref[...] = gain[...] * jax.nn.silu(gate[...].astype(F32))
    keys, running = scan_terms(wd[...], nd[...], wleak[...], nleak[...], spk[...])
    _, width = wd.shape
    q = jnp.concatenate(
        [
            jax.nn.silu(wp[...].astype(F32)) * width ** (-0.5),
            jax.nn.silu(np_[...].astype(F32)) * (width // 2) ** (-0.5),
        ],
        axis=1,
    )
    qf_ref[...] = (q * jnp.exp(running[0])).astype(BF16)
    qb_ref[...] = (q * jnp.exp(running[1])).astype(BF16)
    lane = iota((HALF, 2 * width), 1)
    heads = (lane < width, (lane >= width) & (lane < 3 * width // 2), lane >= 3 * width // 2)
    row, col = iota((HALF, HALF), 0), iota((HALF, HALF), 1)

    def pair(d, t, s, ref):
        rt = running[d][t * HALF : (t + 1) * HALF]
        rs = running[d][s * HALF : (s + 1) * HALF]
        base = running[d][ref : ref + 1]
        qs = q[t * HALF : (t + 1) * HALF] * jnp.exp(rt - base)
        ks = (keys[d][s * HALF : (s + 1) * HALF] * jnp.exp(base - rs)).astype(BF16)
        return qs, ks

    mid = HALF // 2
    terms = {
        (0, 0): [(0, pair(0, 0, 0, mid - 1)), (1, pair(1, 0, 0, mid))],
        (1, 1): [(0, pair(0, 1, 1, HALF + mid - 1)), (1, pair(1, 1, 1, HALF + mid))],
        (1, 0): [(None, pair(0, 1, 0, HALF - 1))],
        (0, 1): [(None, pair(1, 0, 1, HALF))],
    }

    def scores(block, head):
        total = None
        for d, (qs, ks) in terms[block]:
            lo = 0 if head == 0 else width
            picked = jnp.where(heads[head], qs, 0.0)[:, lo : lo + width].astype(BF16)
            part = dot(picked, ks[:, lo : lo + width], (1, 1))
            if d is not None:
                part = jnp.where(row >= col if d == 0 else row <= col, part, 0.0)
            total = part if total is None else total + part
        return total

    for head in range(3):
        full = jnp.concatenate(
            [
                jnp.concatenate([scores((0, 0), head), scores((0, 1), head)], axis=1),
                jnp.concatenate([scores((1, 0), head), scores((1, 1), head)], axis=1),
            ],
            axis=0,
        ).astype(BF16)
        at = slice(head * width, (head + 1) * width)
        o_ref[:, at] = dot(full, v[:, at])
    fetch.wait()


def pick_column(block, d, member):
    width = block.shape[1]
    per = width // SLICE
    rows = block.astype(F32)
    wide = rows[4 * d : 4 * d + 1] + rows[4 * d + 1 : 4 * d + 2]
    slim = rows[4 * d + 2 : 4 * d + 3] + rows[4 * d + 3 : 4 * d + 4]
    row = jnp.where(member >= per, slim, wide)
    want = iota((SLICE, width), 0) + SLICE * (member % per)
    hit = iota((SLICE, width), 1) == want
    return jnp.sum(jnp.where(hit, row, 0.0), axis=1, keepdims=True)


def group_kernel(place, got, pre_ref, dec_ref, tot_ref):
    member = place[1]
    count, _, width = got.shape
    summed = jnp.zeros((16, width), F32)
    for i in range(count):
        summed = summed + got[i, 2 * SLICE :, :].astype(F32)
    for d in range(2):
        at = slice(d * SLICE, (d + 1) * SLICE)
        state = jnp.zeros((SLICE, width), F32)
        total = jnp.zeros((SLICE, 1), F32)
        for i in range(count) if d == 0 else reversed(range(count)):
            pre_ref[i, at, :] = state
            dec_ref[i, at, :] = jnp.broadcast_to(jnp.exp(total), (SLICE, width))
            column = pick_column(got[i, 2 * SLICE :, :], d, member)
            state = jnp.exp(column) * state + got[i, at, :].astype(F32)
            total = total + column
        for g in range(tot_ref.shape[0]):
            tot_ref[g, at, :] = state.astype(BF16)
    rows = [summed[2 * n : 2 * n + 1] + summed[2 * n + 1 : 2 * n + 2] for n in range(4)]
    block = decay_rows(rows)
    for g in range(tot_ref.shape[0]):
        tot_ref[g, 2 * SLICE :, :] = block


def carry_kernel(place, totals, pre, dec, out):
    group, member = place[0], place[1]
    count, _, width = pre.shape
    groups = totals.shape[0]
    for d in range(2):
        at = slice(d * SLICE, (d + 1) * SLICE)
        carry = jnp.zeros((SLICE, width), F32)
        for g in range(groups) if d == 0 else reversed(range(groups)):
            column = pick_column(totals[g, 2 * SLICE :, :], d, member)
            moved = jnp.exp(column) * carry + totals[g, at, :].astype(F32)
            carry = jnp.where(g < group if d == 0 else g > group, moved, carry)
        for i in range(count):
            out[i, at, :] = (pre[i, at, :] + dec[i, at, :] * carry).astype(BF16)


def mix_kernel(states, o_ref, qf, qb, scale, proj, out):
    n, width = o_ref.shape[0], states.shape[2]
    members = states.shape[0]
    entering = [
        jnp.concatenate(
            [states[j, d * SLICE : (d + 1) * SLICE, :] for j in range(members)], axis=0
        )
        for d in range(2)
    ]
    low = iota((n, width), 1) < width // 2
    mixed = []
    for head in range(3):
        at = slice(head * width, (head + 1) * width)
        total = o_ref[:, at]
        for d, q in enumerate((qf, qb)):
            if head == 0:
                total = total + dot(q[:, :width], entering[d][:width])
            else:
                keep = low if head == 1 else jnp.logical_not(low)
                own = jnp.where(keep, q[:, width:].astype(F32), 0.0).astype(BF16)
                total = total + dot(own, entering[d][width:])
        total = total * lax.rsqrt(jnp.mean(total * total, axis=1, keepdims=True) + EPS)
        total = total * scale[:, at]
        mixed.append(total.astype(BF16))
    out[...] = dot(jnp.concatenate(mixed, axis=1), proj[...]).astype(BF16)


def slot_matrix(routes):
    rows = routes.shape[1]
    slots = 32 * CAP
    expert = iota((slots, rows), 0) // CAP
    first = routes[0:1] == expert
    second = routes[1:2] == expert
    named = jnp.logical_or(first, second)
    before = (iota((rows, rows), 0) < iota((rows, rows), 1)).astype(F32).astype(BF16)
    rank = dot(named.astype(F32).astype(BF16), before)
    placed = rank.astype(jnp.int32) == iota((slots, rows), 0) % CAP
    return jnp.logical_and(first, placed), jnp.logical_and(second, placed)


def route_kernel(routes, share, skip, gain, chosen_ref, hi_ref, lo_ref, skip_ref, gain_ref):
    skip_ref[...] = skip[...]
    gain_ref[...] = gain[...]
    first, second = slot_matrix(routes[...])
    chosen_ref[...] = jnp.logical_or(first, second).astype(F32).astype(BF16)
    weight = jnp.where(first, share[0:1], 0.0) + jnp.where(second, share[1:2], 0.0)
    hi_ref[...], lo_ref[...] = split_parts(weight)


def dispatch_kernel(parts, skip, gain, chosen, hidden_ref, out):
    mixing = parts[0].astype(F32)
    for k in range(1, parts.shape[0]):
        mixing = mixing + parts[k].astype(F32)
    hidden_bf = (skip[...].astype(F32) + mixing).astype(BF16)
    hidden_ref[...] = hidden_bf
    hidden = hidden_bf.astype(F32)
    normed = hidden * lax.rsqrt(jnp.mean(hidden * hidden, axis=1, keepdims=True) + EPS)
    normed = (normed * gain[...]).astype(BF16)
    out[...] = block_of(dot(chosen[...], normed).astype(BF16))


def rows_of(block):
    return block.astype(F32).reshape(-1, block.shape[-1]).astype(BF16)


def block_of(rows):
    return rows.astype(F32).reshape(-1, CAP, rows.shape[-1]).astype(BF16)


def split_kernel(got, low, high):
    half = got.shape[0] // 2
    low[...] = rows_of(got[:half])
    high[...] = rows_of(got[half:])


def own_kernel(low, high, a, b, c, part_low, part_high, wg, wu, wd, sems):
    moves = [
        pltpu.make_async_copy(src, dst, sems.at[n])
        for n, (src, dst) in enumerate(((a, wg), (b, wu), (c, wd)))
    ]
    for move in moves:
        move.start()
    rows = jnp.concatenate([low[...], high[...]], axis=0)
    moves[0].wait()
    gate = jax.nn.silu(dot(rows, wg[...]))
    moves[1].wait()
    act = (gate * dot(rows, wu[...])).astype(BF16)
    moves[2].wait()
    part = dot(act, wd[...]).astype(BF16)
    half = low.shape[0]
    part_low[...] = part[:half]
    part_high[...] = part[half:]


def piece_kernel(x, y, wg, wu, wd, out_x, out_y):
    rows = jnp.concatenate([x[...], y[...]], axis=0)
    act = (jax.nn.silu(dot(rows, wg[...])) * dot(rows, wu[...])).astype(BF16)
    part = dot(act, wd[...]).astype(BF16)
    half = x.shape[0]
    out_x[...] = part[:half]
    out_y[...] = part[half:]


def add_kernel(a, b, out):
    out[...] = (a[...].astype(F32) + b[...].astype(F32)).astype(BF16)


def sum_kernel(low_a, low_b, low_c, high_a, high_b, high_c, out):
    half = out.shape[0] // 2
    f = lambda ref: ref[...].astype(F32)
    out[:half] = block_of((f(low_a) + f(low_b) + f(low_c)).astype(BF16))
    out[half:] = block_of((f(high_a) + f(high_b) + f(high_c)).astype(BF16))


def combine_kernel(hidden, back, hi, lo, out):
    rows = rows_of(back[...])
    mixture = dot(hi[...], rows, (0, 0)) + dot(lo[...], rows, (0, 0))
    out[...] = (hidden[...].astype(F32) + mixture).astype(BF16)


def sds(shape, dtype):
    return jax.ShapeDtypeStruct(shape, dtype)


def near(shape, dtype):
    return pltpu.VMEM(shape, dtype)


def nearby(*arrays):
    return tuple(pltpu.with_memory_space_constraint(a, pltpu.VMEM) for a in arrays)


def params(mib=24):
    return pltpu.CompilerParams(vmem_limit_bytes=mib << 20)


def distant(*arrays):
    return tuple(pltpu.with_memory_space_constraint(a, pltpu.HBM) for a in arrays)


VMEM = pl.BlockSpec(memory_space=pltpu.VMEM)
SMEM = pl.BlockSpec(memory_space=pltpu.SMEM)


def cost(flops):
    return pl.CostEstimate(flops=flops, bytes_accessed=1 << 20, transcendentals=0)


def local(
    skip_stream,
    wide_probe_logits,
    narrow_probe_logits,
    wide_decay_logits,
    narrow_decay_logits,
    wide_floor_complement,
    narrow_floor_complement,
    payloads,
    result_switch_logits,
    spike_decays,
    channel_scale_vector,
    result_mapping_matrix,
    specialist_scale_vector,
    assignments,
    assignment_share,
    specialist_switch_matrix,
    specialist_raising_matrix,
    specialist_lowering_matrix,
):
    tokens, width = wide_probe_logits.shape
    rows, model = skip_stream.shape
    joint = payloads.shape[1]
    members = lax.axis_size(ZG)
    groups = lax.axis_size("zh")
    shards = lax.axis_size("tp")
    experts = lax.axis_size(SP)
    place = jnp.stack([lax.axis_index("zh"), lax.axis_index(ZG)]).astype(jnp.int32)
    decay_args = (
        wide_decay_logits,
        narrow_decay_logits,
        wide_floor_complement,
        narrow_floor_complement,
        payloads,
        spike_decays.T,
    )

    summary = pl.pallas_call(
        summary_kernel,
        out_shape=near((members, PAY, width), BF16),
        compiler_params=params(),
        cost_estimate=cost(4 << 20),
    )(*distant(*decay_args))
    by_slice = lax.all_to_all(summary, ZG, 0, 0, tiled=True)
    slots = experts * CAP
    head_gain = channel_scale_vector.reshape(1, joint)
    chosen, share_hi, share_lo, skip, norm_gain = pl.pallas_call(
        route_kernel,
        out_shape=[near((slots, rows), BF16)] * 3
        + [near((rows, model), BF16), near((1, model), F32)],
        compiler_params=params(),
        cost_estimate=cost(1 << 20),
    )(
        *distant(
            assignments.T,
            assignment_share.T,
            skip_stream,
            specialist_scale_vector.reshape(1, model),
        )
    )
    inside, q_fwd, q_bwd, scale, projection = pl.pallas_call(
        local_kernel,
        in_specs=[VMEM] * 10 + [pl.BlockSpec(memory_space=pl.ANY)],
        out_shape=[
            near((tokens, joint), F32),
            near((tokens, 2 * width), BF16),
            near((tokens, 2 * width), BF16),
            near((tokens, joint), F32),
            near(result_mapping_matrix.shape, BF16),
        ],
        scratch_shapes=[pltpu.SemaphoreType.DMA],
        compiler_params=params(),
        cost_estimate=cost(64 << 20),
    )(
        *distant(
            wide_probe_logits,
            narrow_probe_logits,
            *decay_args,
            result_switch_logits,
            head_gain,
            result_mapping_matrix,
        )
    )
    before, decayed, total = pl.pallas_call(
        group_kernel,
        in_specs=[SMEM, VMEM],
        out_shape=[
            near((members, 2 * SLICE, width), F32),
            near((members, 2 * SLICE, width), F32),
            near((groups, PAY, width), BF16),
        ],
        compiler_params=params(),
        cost_estimate=cost(4 << 20),
    )(place, *nearby(by_slice))
    came = lax.all_to_all(total, "zh", 0, 0, tiled=True)
    carried = pl.pallas_call(
        carry_kernel,
        in_specs=[SMEM] + [VMEM] * 3,
        out_shape=near((members, 2 * SLICE, width), BF16),
        compiler_params=params(),
        cost_estimate=cost(4 << 20),
    )(place, *nearby(came, before, decayed))
    entering = lax.all_to_all(carried, ZG, 0, 0, tiled=True)
    mixed = pl.pallas_call(
        mix_kernel,
        out_shape=near((tokens, model), BF16),
        compiler_params=params(),
        cost_estimate=cost(256 << 20),
    )(*nearby(entering, inside, q_fwd, q_bwd, scale, projection))
    parts = lax.all_to_all(mixed.reshape(shards, rows, model), "tp", 0, 0, tiled=True)
    hidden, outgoing = pl.pallas_call(
        dispatch_kernel,
        out_shape=[near((rows, model), BF16), near((experts, CAP, model), BF16)],
        compiler_params=params(),
        cost_estimate=cost(16 << 20),
    )(*nearby(parts, skip, norm_gain, chosen))
    own = lax.all_to_all(outgoing, SP, 0, 0, tiled=True)

    up_ring = [(i, (i + 1) % shards) for i in range(shards)]
    down_ring = [(i, (i - 1) % shards) for i in range(shards)]

    def up(x):
        return lax.ppermute(x, "tp", up_ring)

    def down(x):
        return lax.ppermute(x, "tp", down_ring)

    half = slots // 2
    piece = near((half, model), BF16)

    def call(kernel, flops, *arrays, **rest):
        rest = {"out_shape": piece, **rest}
        return pl.pallas_call(
            kernel, compiler_params=params(), cost_estimate=cost(flops), **rest
        )(*arrays)

    weights = (
        specialist_switch_matrix[0],
        specialist_raising_matrix[0],
        specialist_lowering_matrix[0],
    )
    own_low, own_high = call(split_kernel, 1 << 20, *nearby(own), out_shape=[piece] * 2)
    left_low, right_high = up(own_low), down(own_high)
    left_high, right_low = up(own_high), down(own_low)
    sum_low, sum_high, *weights = call(
        own_kernel,
        2 << 30,
        *nearby(own_low, own_high),
        *distant(*weights),
        in_specs=[VMEM] * 2 + [pl.BlockSpec(memory_space=pl.ANY)] * 3,
        out_shape=[piece] * 2 + [near(w.shape, w.dtype) for w in weights],
        scratch_shapes=[pltpu.SemaphoreType.DMA((3,))],
    )

    def part(x, y):
        return call(piece_kernel, 2 << 30, *nearby(x, y, *weights), out_shape=[piece] * 2)

    def add(a, b):
        return call(add_kernel, 1 << 20, *nearby(a, b))

    far_low, far_high = up(left_low), down(right_high)
    for_left_low, for_right_high = part(left_low, right_high)
    got_high, got_low = up(for_right_high), down(for_left_low)
    for_left_high, for_right_low = part(left_high, right_low)
    for_far_low, for_far_high = part(far_low, far_high)
    add_low, add_high = up(for_far_low), down(for_far_high)
    last_low = up(add(for_right_low, add_low))
    last_high = down(add(for_left_high, add_high))
    summed = call(
        sum_kernel,
        1 << 20,
        *nearby(sum_low, last_low, got_low, sum_high, last_high, got_high),
        out_shape=near((experts, CAP, model), BF16),
    )
    back = lax.all_to_all(summed, SP, 0, 0, tiled=True)
    return pl.pallas_call(
        combine_kernel,
        out_shape=sds((rows, model), BF16),
        compiler_params=params(),
        cost_estimate=cost(16 << 20),
    )(*nearby(hidden, back, share_hi, share_lo))


def solution(mesh):
    torus = Mesh(
        mesh.devices.reshape(mesh.shape["grp"], 4, 4, 2, mesh.shape["tp"]),
        GRP_SP_TP,
    )
    placed = (
        P(GRP_SP_TP, None),
        P(GRP_SP, "tp"),
        P(GRP_SP, "tp"),
        P(GRP_SP, "tp"),
        P(GRP_SP, "tp"),
        P(None, "tp"),
        P(None, "tp"),
        P(GRP_SP, "tp"),
        P(GRP_SP, "tp"),
        P(GRP_SP, "tp"),
        P("tp"),
        P("tp", None),
        P(),
        P(GRP_SP_TP, None),
        P(GRP_SP_TP, None),
        P(SP, None, "tp"),
        P(SP, None, "tp"),
        P(SP, "tp", None),
    )
    return jax.shard_map(
        local, mesh=torus, in_specs=placed, out_specs=P(GRP_SP_TP, None), check_vma=False
    )
```

```python
import jax
import jax.numpy as jnp
from jax import lax
from jax.experimental import pallas as pl
from jax.experimental.pallas import tpu as pltpu
from jax.sharding import Mesh
from jax.sharding import PartitionSpec as P

F32 = jnp.float32
BF16 = jnp.bfloat16
EPS = 1e-06
HALF = 64
SLICE = 32
PAY = 80
CAP = 4
ZG = ("zl", "c")
SP = ("zh", "zl", "c")
GRP_SP = ("grp", "zh", "zl", "c")
GRP_SP_TP = ("grp", "zh", "zl", "c", "tp")


def dot(a, b, contract=(1, 0), precision=None):
    dims = (((contract[0],), (contract[1],)), ((), ()))
    return lax.dot_general(a, b, dims, precision=precision, preferred_element_type=F32)


def iota(shape, axis):
    return lax.broadcasted_iota(jnp.int32, shape, axis)


def split_parts(x):
    hi = x.astype(BF16)
    return hi, (x - hi.astype(F32)).astype(BF16)


def exact_sums(ones, x, side=1):
    hi, rest = x.astype(BF16), x
    parts = [hi]
    for _ in range(2):
        rest = rest - parts[-1].astype(F32)
        parts.append(rest.astype(BF16))
    bits = ones.astype(F32).astype(BF16)
    stacked = jnp.concatenate([p.astype(F32) for p in parts], axis=0).astype(BF16)
    if side == 0:
        return dot(stacked, jnp.concatenate([bits] * 3, axis=0), (0, 0))
    return dot(jnp.concatenate([bits] * 3, axis=1), stacked)


def key_and_decay(logits, leaks, spikes):
    gate = jax.nn.sigmoid(-logits.astype(F32))
    rows = [leaks[d : d + 1] * gate for d in range(2)]
    return rows, [jnp.log1p(-k) + spikes for k in rows]


def scan_terms(wd, nd, wleak, nleak, spk):
    n, width = wd.shape
    heads = spk.shape[0]
    lane = iota((heads, 2 * width), 1)
    owner = jnp.where(lane < width, 0, jnp.where(lane < 3 * width // 2, 1, 2))
    spikes = exact_sums(iota((heads, 2 * width), 0) == owner, spk, 0)
    kw, aw = key_and_decay(wd, wleak, spikes[:, :width])
    kn, an = key_and_decay(nd, nleak, spikes[:, width:])
    row, col = iota((n, n), 0), iota((n, n), 1)
    fwd = exact_sums(row >= col, jnp.concatenate([aw[0], an[0]], axis=1))
    bwd = exact_sums(row <= col, jnp.concatenate([aw[1], an[1]], axis=1))
    keys = [jnp.concatenate([kw[d], kn[d]], axis=1) for d in range(2)]
    return keys, (fwd, bwd)


def decay_rows(rows):
    width = rows[0].shape[1]
    at = iota((16, width), 0)
    block = jnp.zeros((16, width), F32)
    for n, row in enumerate(rows):
        hi = row.astype(BF16).astype(F32)
        block = jnp.where(at == 2 * n, hi, block)
        block = jnp.where(at == 2 * n + 1, row - hi, block)
    return block.astype(BF16)


def summary_kernel(wd, nd, wleak, nleak, v, spk, out):
    keys, running = scan_terms(wd[...], nd[...], wleak[...], nleak[...], spk[...])
    n, width = wd.shape
    values = v[...]
    last = (n - 1, 0)
    rows = []
    for d in range(2):
        closing = running[d][last[d] : last[d] + 1]
        fresh = (keys[d] * jnp.exp(closing - running[d])).astype(BF16)
        wide = dot(fresh[:, :width], values[:, :width], (0, 0))
        both = dot(fresh[:, width:], values[:, width:], (0, 0))
        slim = jnp.where(iota((width, width), 0) < width // 2, both[:, :width], both[:, width:])
        state = jnp.concatenate([wide, slim], axis=0).astype(BF16)
        for j in range(out.shape[0]):
            out[j, d * SLICE : (d + 1) * SLICE, :] = state[j * SLICE : (j + 1) * SLICE]
        rows += [closing[:, :width], closing[:, width:]]
    block = decay_rows(rows)
    for j in range(out.shape[0]):
        out[j, 2 * SLICE :, :] = block


def local_kernel(
    wp, np_, wd, nd, wleak, nleak, v, spk, gate, gain, proj_far, o_ref, qf_ref, qb_ref, scale_ref, proj, sem
):
    fetch = pltpu.make_async_copy(proj_far, proj, sem)
    fetch.start()
    scale_ref[...] = gain[...] * jax.nn.silu(gate[...].astype(F32))
    keys, running = scan_terms(wd[...], nd[...], wleak[...], nleak[...], spk[...])
    _, width = wd.shape
    q = jnp.concatenate(
        [
            jax.nn.silu(wp[...].astype(F32)) * width ** (-0.5),
            jax.nn.silu(np_[...].astype(F32)) * (width // 2) ** (-0.5),
        ],
        axis=1,
    )
    qf_ref[...] = (q * jnp.exp(running[0])).astype(BF16)
    qb_ref[...] = (q * jnp.exp(running[1])).astype(BF16)
    lane = iota((HALF, 2 * width), 1)
    heads = (lane < width, (lane >= width) & (lane < 3 * width // 2), lane >= 3 * width // 2)
    row, col = iota((HALF, HALF), 0), iota((HALF, HALF), 1)

    def pair(d, t, s, ref):
        rt = running[d][t * HALF : (t + 1) * HALF]
        rs = running[d][s * HALF : (s + 1) * HALF]
        base = running[d][ref : ref + 1]
        qs = q[t * HALF : (t + 1) * HALF] * jnp.exp(rt - base)
        ks = (keys[d][s * HALF : (s + 1) * HALF] * jnp.exp(base - rs)).astype(BF16)
        return qs, ks

    mid = HALF // 2
    terms = {
        (0, 0): [(0, pair(0, 0, 0, mid - 1)), (1, pair(1, 0, 0, mid))],
        (1, 1): [(0, pair(0, 1, 1, HALF + mid - 1)), (1, pair(1, 1, 1, HALF + mid))],
        (1, 0): [(None, pair(0, 1, 0, HALF - 1))],
        (0, 1): [(None, pair(1, 0, 1, HALF))],
    }

    def scores(block, head):
        total = None
        for d, (qs, ks) in terms[block]:
            lo = 0 if head == 0 else width
            picked = jnp.where(heads[head], qs, 0.0)[:, lo : lo + width].astype(BF16)
            part = dot(picked, ks[:, lo : lo + width], (1, 1))
            if d is not None:
                part = jnp.where(row >= col if d == 0 else row <= col, part, 0.0)
            total = part if total is None else total + part
        return total

    for head in range(3):
        full = jnp.concatenate(
            [
                jnp.concatenate([scores((0, 0), head), scores((0, 1), head)], axis=1),
                jnp.concatenate([scores((1, 0), head), scores((1, 1), head)], axis=1),
            ],
            axis=0,
        ).astype(BF16)
        at = slice(head * width, (head + 1) * width)
        o_ref[:, at] = dot(full, v[:, at])
    fetch.wait()


def pick_column(block, d, member):
    width = block.shape[1]
    per = width // SLICE
    rows = block.astype(F32)
    wide = rows[4 * d : 4 * d + 1] + rows[4 * d + 1 : 4 * d + 2]
    slim = rows[4 * d + 2 : 4 * d + 3] + rows[4 * d + 3 : 4 * d + 4]
    row = jnp.where(member >= per, slim, wide)
    want = iota((SLICE, width), 0) + SLICE * (member % per)
    hit = iota((SLICE, width), 1) == want
    return jnp.sum(jnp.where(hit, row, 0.0), axis=1, keepdims=True)


def group_kernel(got, pre_ref, dec_ref, tot_ref):
    member = lax.axis_index(ZG)
    count, _, width = got.shape
    summed = jnp.zeros((16, width), F32)
    for i in range(count):
        summed = summed + got[i, 2 * SLICE :, :].astype(F32)
    for d in range(2):
        at = slice(d * SLICE, (d + 1) * SLICE)
        state = jnp.zeros((SLICE, width), F32)
        total = jnp.zeros((SLICE, 1), F32)
        for i in range(count) if d == 0 else reversed(range(count)):
            pre_ref[i, at, :] = state
            dec_ref[i, at, :] = jnp.broadcast_to(jnp.exp(total), (SLICE, width))
            column = pick_column(got[i, 2 * SLICE :, :], d, member)
            state = jnp.exp(column) * state + got[i, at, :].astype(F32)
            total = total + column
        for g in range(tot_ref.shape[0]):
            tot_ref[g, at, :] = state.astype(BF16)
    rows = [summed[2 * n : 2 * n + 1] + summed[2 * n + 1 : 2 * n + 2] for n in range(4)]
    block = decay_rows(rows)
    for g in range(tot_ref.shape[0]):
        tot_ref[g, 2 * SLICE :, :] = block


def carry_kernel(totals, pre, dec, out):
    group, member = lax.axis_index("zh"), lax.axis_index(ZG)
    count, _, width = pre.shape
    groups = totals.shape[0]
    for d in range(2):
        at = slice(d * SLICE, (d + 1) * SLICE)
        carry = jnp.zeros((SLICE, width), F32)
        for g in range(groups) if d == 0 else reversed(range(groups)):
            column = pick_column(totals[g, 2 * SLICE :, :], d, member)
            moved = jnp.exp(column) * carry + totals[g, at, :].astype(F32)
            carry = jnp.where(g < group if d == 0 else g > group, moved, carry)
        for i in range(count):
            out[i, at, :] = (pre[i, at, :] + dec[i, at, :] * carry).astype(BF16)


def mix_kernel(states, o_ref, qf, qb, scale, proj, out):
    n, width = o_ref.shape[0], states.shape[2]
    members = states.shape[0]
    entering = [
        jnp.concatenate(
            [states[j, d * SLICE : (d + 1) * SLICE, :] for j in range(members)], axis=0
        )
        for d in range(2)
    ]
    low = iota((n, width), 1) < width // 2
    mixed = []
    for head in range(3):
        at = slice(head * width, (head + 1) * width)
        total = o_ref[:, at]
        for d, q in enumerate((qf, qb)):
            if head == 0:
                total = total + dot(q[:, :width], entering[d][:width])
            else:
                keep = low if head == 1 else jnp.logical_not(low)
                own = jnp.where(keep, q[:, width:].astype(F32), 0.0).astype(BF16)
                total = total + dot(own, entering[d][width:])
        total = total * lax.rsqrt(jnp.mean(total * total, axis=1, keepdims=True) + EPS)
        total = total * scale[:, at]
        mixed.append(total.astype(BF16))
    out[...] = dot(jnp.concatenate(mixed, axis=1), proj[...]).astype(BF16)


def slot_matrix(routes):
    rows = routes.shape[1]
    slots = 32 * CAP
    expert = iota((slots, rows), 0) // CAP
    first = routes[0:1] == expert
    second = routes[1:2] == expert
    named = jnp.logical_or(first, second)
    before = (iota((rows, rows), 0) < iota((rows, rows), 1)).astype(F32).astype(BF16)
    rank = dot(named.astype(F32).astype(BF16), before)
    placed = rank.astype(jnp.int32) == iota((slots, rows), 0) % CAP
    return jnp.logical_and(first, placed), jnp.logical_and(second, placed)


def route_kernel(routes, share, skip, gain, chosen_ref, hi_ref, lo_ref, skip_ref, gain_ref):
    skip_ref[...] = skip[...]
    gain_ref[...] = gain[...]
    first, second = slot_matrix(routes[...])
    chosen_ref[...] = jnp.logical_or(first, second).astype(F32).astype(BF16)
    weight = jnp.where(first, share[0:1], 0.0) + jnp.where(second, share[1:2], 0.0)
    hi_ref[...], lo_ref[...] = split_parts(weight)


def dispatch_kernel(parts, skip, gain, chosen, hidden_ref, out):
    mixing = parts[0].astype(F32)
    for k in range(1, parts.shape[0]):
        mixing = mixing + parts[k].astype(F32)
    hidden_bf = (skip[...].astype(F32) + mixing).astype(BF16)
    hidden_ref[...] = hidden_bf
    hidden = hidden_bf.astype(F32)
    normed = hidden * lax.rsqrt(jnp.mean(hidden * hidden, axis=1, keepdims=True) + EPS)
    normed = (normed * gain[...]).astype(BF16)
    out[...] = block_of(dot(chosen[...], normed).astype(BF16))


def rows_of(block):
    return block.astype(F32).reshape(-1, block.shape[-1]).astype(BF16)


def block_of(rows):
    return rows.astype(F32).reshape(-1, CAP, rows.shape[-1]).astype(BF16)


def split_kernel(got, low, high):
    half = got.shape[0] // 2
    low[...] = rows_of(got[:half])
    high[...] = rows_of(got[half:])


def own_kernel(low, high, a, b, c, part_low, part_high, wg, wu, wd, sems):
    moves = [
        pltpu.make_async_copy(src, dst, sems.at[n])
        for n, (src, dst) in enumerate(((a, wg), (b, wu), (c, wd)))
    ]
    for move in moves:
        move.start()
    rows = jnp.concatenate([low[...], high[...]], axis=0)
    moves[0].wait()
    gate = jax.nn.silu(dot(rows, wg[...]))
    moves[1].wait()
    act = (gate * dot(rows, wu[...])).astype(BF16)
    moves[2].wait()
    part = dot(act, wd[...]).astype(BF16)
    half = low.shape[0]
    part_low[...] = part[:half]
    part_high[...] = part[half:]


def piece_kernel(x, y, wg, wu, wd, out_x, out_y):
    rows = jnp.concatenate([x[...], y[...]], axis=0)
    act = (jax.nn.silu(dot(rows, wg[...])) * dot(rows, wu[...])).astype(BF16)
    part = dot(act, wd[...]).astype(BF16)
    half = x.shape[0]
    out_x[...] = part[:half]
    out_y[...] = part[half:]


def add_kernel(a, b, out):
    out[...] = (a[...].astype(F32) + b[...].astype(F32)).astype(BF16)


def sum_kernel(low_a, low_b, low_c, high_a, high_b, high_c, out):
    half = out.shape[0] // 2
    f = lambda ref: ref[...].astype(F32)
    out[:half] = block_of((f(low_a) + f(low_b) + f(low_c)).astype(BF16))
    out[half:] = block_of((f(high_a) + f(high_b) + f(high_c)).astype(BF16))


def combine_kernel(hidden, back, hi, lo, out):
    rows = rows_of(back[...])
    mixture = dot(hi[...], rows, (0, 0)) + dot(lo[...], rows, (0, 0))
    out[...] = (hidden[...].astype(F32) + mixture).astype(BF16)


def sds(shape, dtype):
    return jax.ShapeDtypeStruct(shape, dtype)


def near(shape, dtype):
    return pltpu.VMEM(shape, dtype)


def nearby(*arrays):
    return tuple(pltpu.with_memory_space_constraint(a, pltpu.VMEM) for a in arrays)


def params(mib=24):
    return pltpu.CompilerParams(vmem_limit_bytes=mib << 20)


def distant(*arrays):
    return tuple(pltpu.with_memory_space_constraint(a, pltpu.HBM) for a in arrays)


VMEM = pl.BlockSpec(memory_space=pltpu.VMEM)


def cost(flops):
    return pl.CostEstimate(flops=flops, bytes_accessed=1 << 20, transcendentals=0)


def local(
    skip_stream,
    wide_probe_logits,
    narrow_probe_logits,
    wide_decay_logits,
    narrow_decay_logits,
    wide_floor_complement,
    narrow_floor_complement,
    payloads,
    result_switch_logits,
    spike_decays,
    channel_scale_vector,
    result_mapping_matrix,
    specialist_scale_vector,
    assignments,
    assignment_share,
    specialist_switch_matrix,
    specialist_raising_matrix,
    specialist_lowering_matrix,
):
    tokens, width = wide_probe_logits.shape
    rows, model = skip_stream.shape
    joint = payloads.shape[1]
    members = lax.axis_size(ZG)
    groups = lax.axis_size("zh")
    shards = lax.axis_size("tp")
    experts = lax.axis_size(SP)
    decay_args = (
        wide_decay_logits,
        narrow_decay_logits,
        wide_floor_complement,
        narrow_floor_complement,
        payloads,
        spike_decays.T,
    )

    summary = pl.pallas_call(
        summary_kernel,
        out_shape=near((members, PAY, width), BF16),
        compiler_params=params(),
        cost_estimate=cost(4 << 20),
    )(*distant(*decay_args))
    by_slice = lax.all_to_all(summary, ZG, 0, 0, tiled=True)
    slots = experts * CAP
    head_gain = channel_scale_vector.reshape(1, joint)
    chosen, share_hi, share_lo, skip, norm_gain = pl.pallas_call(
        route_kernel,
        out_shape=[near((slots, rows), BF16)] * 3
        + [near((rows, model), BF16), near((1, model), F32)],
        compiler_params=params(),
        cost_estimate=cost(1 << 20),
    )(
        *distant(
            assignments.T,
            assignment_share.T,
            skip_stream,
            specialist_scale_vector.reshape(1, model),
        )
    )
    inside, q_fwd, q_bwd, scale, projection = pl.pallas_call(
        local_kernel,
        in_specs=[VMEM] * 10 + [pl.BlockSpec(memory_space=pl.ANY)],
        out_shape=[
            near((tokens, joint), F32),
            near((tokens, 2 * width), BF16),
            near((tokens, 2 * width), BF16),
            near((tokens, joint), F32),
            near(result_mapping_matrix.shape, BF16),
        ],
        scratch_shapes=[pltpu.SemaphoreType.DMA],
        compiler_params=params(),
        cost_estimate=cost(64 << 20),
    )(
        *distant(
            wide_probe_logits,
            narrow_probe_logits,
            *decay_args,
            result_switch_logits,
            head_gain,
            result_mapping_matrix,
        )
    )
    before, decayed, total = pl.pallas_call(
        group_kernel,
        out_shape=[
            near((members, 2 * SLICE, width), F32),
            near((members, 2 * SLICE, width), F32),
            near((groups, PAY, width), BF16),
        ],
        compiler_params=params(),
        cost_estimate=cost(4 << 20),
    )(*nearby(by_slice))
    came = lax.all_to_all(total, "zh", 0, 0, tiled=True)
    carried = pl.pallas_call(
        carry_kernel,
        out_shape=near((members, 2 * SLICE, width), BF16),
        compiler_params=params(),
        cost_estimate=cost(4 << 20),
    )(*nearby(came, before, decayed))
    entering = lax.all_to_all(carried, ZG, 0, 0, tiled=True)
    mixed = pl.pallas_call(
        mix_kernel,
        out_shape=near((tokens, model), BF16),
        compiler_params=params(),
        cost_estimate=cost(256 << 20),
    )(*nearby(entering, inside, q_fwd, q_bwd, scale, projection))
    parts = lax.all_to_all(mixed.reshape(shards, rows, model), "tp", 0, 0, tiled=True)
    hidden, outgoing = pl.pallas_call(
        dispatch_kernel,
        out_shape=[near((rows, model), BF16), near((experts, CAP, model), BF16)],
        compiler_params=params(),
        cost_estimate=cost(16 << 20),
    )(*nearby(parts, skip, norm_gain, chosen))
    own = lax.all_to_all(outgoing, SP, 0, 0, tiled=True)

    up_ring = [(i, (i + 1) % shards) for i in range(shards)]
    down_ring = [(i, (i - 1) % shards) for i in range(shards)]

    def up(x):
        return lax.ppermute(x, "tp", up_ring)

    def down(x):
        return lax.ppermute(x, "tp", down_ring)

    half = slots // 2
    piece = near((half, model), BF16)

    def call(kernel, flops, *arrays, **rest):
        rest = {"out_shape": piece, **rest}
        return pl.pallas_call(
            kernel, compiler_params=params(), cost_estimate=cost(flops), **rest
        )(*arrays)

    weights = (
        specialist_switch_matrix[0],
        specialist_raising_matrix[0],
        specialist_lowering_matrix[0],
    )
    own_low, own_high = call(split_kernel, 1 << 20, *nearby(own), out_shape=[piece] * 2)
    left_low, right_high = up(own_low), down(own_high)
    left_high, right_low = up(own_high), down(own_low)
    sum_low, sum_high, *weights = call(
        own_kernel,
        2 << 30,
        *nearby(own_low, own_high),
        *distant(*weights),
        in_specs=[VMEM] * 2 + [pl.BlockSpec(memory_space=pl.ANY)] * 3,
        out_shape=[piece] * 2 + [near(w.shape, w.dtype) for w in weights],
        scratch_shapes=[pltpu.SemaphoreType.DMA((3,))],
    )

    def part(x, y):
        return call(piece_kernel, 2 << 30, *nearby(x, y, *weights), out_shape=[piece] * 2)

    def add(a, b):
        return call(add_kernel, 1 << 20, *nearby(a, b))

    far_low, far_high = up(left_low), down(right_high)
    for_left_low, for_right_high = part(left_low, right_high)
    got_high, got_low = up(for_right_high), down(for_left_low)
    for_left_high, for_right_low = part(left_high, right_low)
    for_far_low, for_far_high = part(far_low, far_high)
    add_low, add_high = up(for_far_low), down(for_far_high)
    last_low = up(add(for_right_low, add_low))
    last_high = down(add(for_left_high, add_high))
    summed = call(
        sum_kernel,
        1 << 20,
        *nearby(sum_low, last_low, got_low, sum_high, last_high, got_high),
        out_shape=near((experts, CAP, model), BF16),
    )
    back = lax.all_to_all(summed, SP, 0, 0, tiled=True)
    return pl.pallas_call(
        combine_kernel,
        out_shape=sds((rows, model), BF16),
        compiler_params=params(),
        cost_estimate=cost(16 << 20),
    )(*nearby(hidden, back, share_hi, share_lo))


def solution(mesh):
    torus = Mesh(
        mesh.devices.reshape(mesh.shape["grp"], 4, 4, 2, mesh.shape["tp"]),
        GRP_SP_TP,
    )
    placed = (
        P(GRP_SP_TP, None),
        P(GRP_SP, "tp"),
        P(GRP_SP, "tp"),
        P(GRP_SP, "tp"),
        P(GRP_SP, "tp"),
        P(None, "tp"),
        P(None, "tp"),
        P(GRP_SP, "tp"),
        P(GRP_SP, "tp"),
        P(GRP_SP, "tp"),
        P("tp"),
        P("tp", None),
        P(),
        P(GRP_SP_TP, None),
        P(GRP_SP_TP, None),
        P(SP, None, "tp"),
        P(SP, None, "tp"),
        P(SP, "tp", None),
    )
    return jax.shard_map(
        local, mesh=torus, in_specs=placed, out_specs=P(GRP_SP_TP, None), check_vma=False
    )
```

```python
import jax
import jax.numpy as jnp
from jax import lax
from jax.experimental import pallas as pl
from jax.experimental.pallas import tpu as pltpu
from jax.sharding import Mesh
from jax.sharding import PartitionSpec as P

F32 = jnp.float32
BF16 = jnp.bfloat16
EPS = 1e-06
HALF = 64
SLICE = 32
PAY = 80
CAP = 4
ZG = ("zl", "c")
SP = ("zh", "zl", "c")
GRP_SP = ("grp", "zh", "zl", "c")
GRP_SP_TP = ("grp", "zh", "zl", "c", "tp")


def dot(a, b, contract=(1, 0), precision=None):
    dims = (((contract[0],), (contract[1],)), ((), ()))
    return lax.dot_general(a, b, dims, precision=precision, preferred_element_type=F32)


def iota(shape, axis):
    return lax.broadcasted_iota(jnp.int32, shape, axis)


def split_parts(x):
    hi = x.astype(BF16)
    return hi, (x - hi.astype(F32)).astype(BF16)


def exact_sums(ones, x, side=1):
    hi, rest = x.astype(BF16), x
    parts = [hi]
    for _ in range(2):
        rest = rest - parts[-1].astype(F32)
        parts.append(rest.astype(BF16))
    bits = ones.astype(F32).astype(BF16)
    stacked = jnp.concatenate([p.astype(F32) for p in parts], axis=0).astype(BF16)
    if side == 0:
        return dot(stacked, jnp.concatenate([bits] * 3, axis=0), (0, 0))
    return dot(jnp.concatenate([bits] * 3, axis=1), stacked)


def key_and_decay(logits, leaks, spikes):
    gate = jax.nn.sigmoid(-logits.astype(F32))
    rows = [leaks[d : d + 1] * gate for d in range(2)]
    return rows, [jnp.log1p(-k) + spikes for k in rows]


def scan_terms(wd, nd, wleak, nleak, spk):
    n, width = wd.shape
    heads = spk.shape[0]
    lane = iota((heads, 2 * width), 1)
    owner = jnp.where(lane < width, 0, jnp.where(lane < 3 * width // 2, 1, 2))
    spikes = exact_sums(iota((heads, 2 * width), 0) == owner, spk, 0)
    kw, aw = key_and_decay(wd, wleak, spikes[:, :width])
    kn, an = key_and_decay(nd, nleak, spikes[:, width:])
    row, col = iota((n, n), 0), iota((n, n), 1)
    fwd = exact_sums(row >= col, jnp.concatenate([aw[0], an[0]], axis=1))
    bwd = exact_sums(row <= col, jnp.concatenate([aw[1], an[1]], axis=1))
    keys = [jnp.concatenate([kw[d], kn[d]], axis=1) for d in range(2)]
    return keys, (fwd, bwd)


def decay_rows(rows):
    width = rows[0].shape[1]
    at = iota((16, width), 0)
    block = jnp.zeros((16, width), F32)
    for n, row in enumerate(rows):
        hi = row.astype(BF16).astype(F32)
        block = jnp.where(at == 2 * n, hi, block)
        block = jnp.where(at == 2 * n + 1, row - hi, block)
    return block.astype(BF16)


def summary_kernel(wd, nd, wleak, nleak, v, spk, out):
    keys, running = scan_terms(wd[...], nd[...], wleak[...], nleak[...], spk[...])
    n, width = wd.shape
    values = v[...]
    last = (n - 1, 0)
    rows = []
    for d in range(2):
        closing = running[d][last[d] : last[d] + 1]
        fresh = (keys[d] * jnp.exp(closing - running[d])).astype(BF16)
        wide = dot(fresh[:, :width], values[:, :width], (0, 0))
        both = dot(fresh[:, width:], values[:, width:], (0, 0))
        slim = jnp.where(iota((width, width), 0) < width // 2, both[:, :width], both[:, width:])
        state = jnp.concatenate([wide, slim], axis=0).astype(BF16)
        for j in range(out.shape[0]):
            out[j, d * SLICE : (d + 1) * SLICE, :] = state[j * SLICE : (j + 1) * SLICE]
        rows += [closing[:, :width], closing[:, width:]]
    block = decay_rows(rows)
    for j in range(out.shape[0]):
        out[j, 2 * SLICE :, :] = block


def local_kernel(
    wp, np_, wd, nd, wleak, nleak, v, spk, gate, gain, proj_far, o_ref, qf_ref, qb_ref, scale_ref, proj, sem
):
    fetch = pltpu.make_async_copy(proj_far, proj, sem)
    fetch.start()
    scale_ref[...] = gain[...] * jax.nn.silu(gate[...].astype(F32))
    keys, running = scan_terms(wd[...], nd[...], wleak[...], nleak[...], spk[...])
    _, width = wd.shape
    q = jnp.concatenate(
        [
            jax.nn.silu(wp[...].astype(F32)) * width ** (-0.5),
            jax.nn.silu(np_[...].astype(F32)) * (width // 2) ** (-0.5),
        ],
        axis=1,
    )
    qf_ref[...] = (q * jnp.exp(running[0])).astype(BF16)
    qb_ref[...] = (q * jnp.exp(running[1])).astype(BF16)
    lane = iota((HALF, 2 * width), 1)
    heads = (lane < width, (lane >= width) & (lane < 3 * width // 2), lane >= 3 * width // 2)
    row, col = iota((HALF, HALF), 0), iota((HALF, HALF), 1)

    def pair(d, t, s, ref):
        rt = running[d][t * HALF : (t + 1) * HALF]
        rs = running[d][s * HALF : (s + 1) * HALF]
        base = running[d][ref : ref + 1]
        qs = q[t * HALF : (t + 1) * HALF] * jnp.exp(rt - base)
        ks = (keys[d][s * HALF : (s + 1) * HALF] * jnp.exp(base - rs)).astype(BF16)
        return qs, ks

    mid = HALF // 2
    terms = {
        (0, 0): [(0, pair(0, 0, 0, mid - 1)), (1, pair(1, 0, 0, mid))],
        (1, 1): [(0, pair(0, 1, 1, HALF + mid - 1)), (1, pair(1, 1, 1, HALF + mid))],
        (1, 0): [(None, pair(0, 1, 0, HALF - 1))],
        (0, 1): [(None, pair(1, 0, 1, HALF))],
    }

    def scores(block, head):
        total = None
        for d, (qs, ks) in terms[block]:
            lo = 0 if head == 0 else width
            picked = jnp.where(heads[head], qs, 0.0)[:, lo : lo + width].astype(BF16)
            part = dot(picked, ks[:, lo : lo + width], (1, 1))
            if d is not None:
                part = jnp.where(row >= col if d == 0 else row <= col, part, 0.0)
            total = part if total is None else total + part
        return total

    for head in range(3):
        full = jnp.concatenate(
            [
                jnp.concatenate([scores((0, 0), head), scores((0, 1), head)], axis=1),
                jnp.concatenate([scores((1, 0), head), scores((1, 1), head)], axis=1),
            ],
            axis=0,
        ).astype(BF16)
        at = slice(head * width, (head + 1) * width)
        o_ref[:, at] = dot(full, v[:, at])
    fetch.wait()


def pick_column(block, d, member):
    width = block.shape[1]
    per = width // SLICE
    rows = block.astype(F32)
    wide = rows[4 * d : 4 * d + 1] + rows[4 * d + 1 : 4 * d + 2]
    slim = rows[4 * d + 2 : 4 * d + 3] + rows[4 * d + 3 : 4 * d + 4]
    row = jnp.where(member >= per, slim, wide)
    want = iota((SLICE, width), 0) + SLICE * (member % per)
    hit = iota((SLICE, width), 1) == want
    return jnp.sum(jnp.where(hit, row, 0.0), axis=1, keepdims=True)


def group_kernel(got, pre_ref, dec_ref, tot_ref):
    member = lax.axis_index(ZG)
    count, _, width = got.shape
    summed = jnp.zeros((16, width), F32)
    for i in range(count):
        summed = summed + got[i, 2 * SLICE :, :].astype(F32)
    for d in range(2):
        at = slice(d * SLICE, (d + 1) * SLICE)
        state = jnp.zeros((SLICE, width), F32)
        total = jnp.zeros((SLICE, 1), F32)
        for i in range(count) if d == 0 else reversed(range(count)):
            pre_ref[i, at, :] = state
            dec_ref[i, at, :] = jnp.broadcast_to(jnp.exp(total), (SLICE, width))
            column = pick_column(got[i, 2 * SLICE :, :], d, member)
            state = jnp.exp(column) * state + got[i, at, :].astype(F32)
            total = total + column
        for g in range(tot_ref.shape[0]):
            tot_ref[g, at, :] = state.astype(BF16)
    rows = [summed[2 * n : 2 * n + 1] + summed[2 * n + 1 : 2 * n + 2] for n in range(4)]
    block = decay_rows(rows)
    for g in range(tot_ref.shape[0]):
        tot_ref[g, 2 * SLICE :, :] = block


def carry_kernel(totals, pre, dec, out):
    group, member = lax.axis_index("zh"), lax.axis_index(ZG)
    count, _, width = pre.shape
    groups = totals.shape[0]
    for d in range(2):
        at = slice(d * SLICE, (d + 1) * SLICE)
        carry = jnp.zeros((SLICE, width), F32)
        for g in range(groups) if d == 0 else reversed(range(groups)):
            column = pick_column(totals[g, 2 * SLICE :, :], d, member)
            moved = jnp.exp(column) * carry + totals[g, at, :].astype(F32)
            carry = jnp.where(g < group if d == 0 else g > group, moved, carry)
        for i in range(count):
            out[i, at, :] = (pre[i, at, :] + dec[i, at, :] * carry).astype(BF16)


def mix_kernel(states, o_ref, qf, qb, scale, proj, out):
    n, width = o_ref.shape[0], states.shape[2]
    members = states.shape[0]
    entering = [
        jnp.concatenate(
            [states[j, d * SLICE : (d + 1) * SLICE, :] for j in range(members)], axis=0
        )
        for d in range(2)
    ]
    low = iota((n, width), 1) < width // 2
    mixed = []
    for head in range(3):
        at = slice(head * width, (head + 1) * width)
        total = o_ref[:, at]
        for d, q in enumerate((qf, qb)):
            if head == 0:
                total = total + dot(q[:, :width], entering[d][:width])
            else:
                keep = low if head == 1 else jnp.logical_not(low)
                own = jnp.where(keep, q[:, width:].astype(F32), 0.0).astype(BF16)
                total = total + dot(own, entering[d][width:])
        total = total * lax.rsqrt(jnp.mean(total * total, axis=1, keepdims=True) + EPS)
        total = total * scale[:, at]
        mixed.append(total.astype(BF16))
    out[...] = dot(jnp.concatenate(mixed, axis=1), proj[...]).astype(BF16)


def slot_matrix(routes):
    rows = routes.shape[1]
    slots = 32 * CAP
    expert = iota((slots, rows), 0) // CAP
    first = routes[0:1] == expert
    second = routes[1:2] == expert
    named = jnp.logical_or(first, second)
    before = (iota((rows, rows), 0) < iota((rows, rows), 1)).astype(F32).astype(BF16)
    rank = dot(named.astype(F32).astype(BF16), before)
    placed = rank.astype(jnp.int32) == iota((slots, rows), 0) % CAP
    return jnp.logical_and(first, placed), jnp.logical_and(second, placed)


def route_kernel(routes, share, skip, gain, chosen_ref, pair_ref, skip_ref, gain_ref):
    skip_ref[...] = skip[...]
    gain_ref[...] = gain[...]
    first, second = slot_matrix(routes[...])
    chosen_ref[...] = jnp.logical_or(first, second).astype(F32).astype(BF16)
    weight = jnp.where(first, share[0:1], 0.0) + jnp.where(second, share[1:2], 0.0)
    hi, lo = split_parts(weight)
    both = jnp.concatenate([hi.astype(F32), lo.astype(F32)], axis=1)
    pair_ref[...] = both.astype(BF16)


def dispatch_kernel(parts, skip, gain, chosen, hidden_ref, out):
    mixing = parts[0].astype(F32)
    for k in range(1, parts.shape[0]):
        mixing = mixing + parts[k].astype(F32)
    hidden_bf = (skip[...].astype(F32) + mixing).astype(BF16)
    hidden_ref[...] = hidden_bf
    hidden = hidden_bf.astype(F32)
    normed = hidden * lax.rsqrt(jnp.mean(hidden * hidden, axis=1, keepdims=True) + EPS)
    normed = (normed * gain[...]).astype(BF16)
    out[...] = block_of(dot(chosen[...], normed).astype(BF16))


def rows_of(block):
    return block.astype(F32).reshape(-1, block.shape[-1]).astype(BF16)


def block_of(rows):
    return rows.astype(F32).reshape(-1, CAP, rows.shape[-1]).astype(BF16)


def split_kernel(got, low, high):
    half = got.shape[0] // 2
    low[...] = rows_of(got[:half])
    high[...] = rows_of(got[half:])


def own_kernel(low, high, a, b, c, part_low, part_high, wg, wu, wd, sems):
    moves = [
        pltpu.make_async_copy(src, dst, sems.at[n])
        for n, (src, dst) in enumerate(((a, wg), (b, wu), (c, wd)))
    ]
    for move in moves:
        move.start()
    rows = jnp.concatenate([low[...], high[...]], axis=0)
    moves[0].wait()
    gate = jax.nn.silu(dot(rows, wg[...]))
    moves[1].wait()
    act = (gate * dot(rows, wu[...])).astype(BF16)
    moves[2].wait()
    part = dot(act, wd[...]).astype(BF16)
    half = low.shape[0]
    part_low[...] = part[:half]
    part_high[...] = part[half:]


def piece_kernel(x, y, wg, wu, wd, out_x, out_y):
    rows = jnp.concatenate([x[...], y[...]], axis=0)
    act = (jax.nn.silu(dot(rows, wg[...])) * dot(rows, wu[...])).astype(BF16)
    part = dot(act, wd[...]).astype(BF16)
    half = x.shape[0]
    out_x[...] = part[:half]
    out_y[...] = part[half:]


def add_kernel(a, b, out):
    out[...] = (a[...].astype(F32) + b[...].astype(F32)).astype(BF16)


def sum_kernel(low_a, low_b, low_c, high_a, high_b, high_c, out):
    half = out.shape[0] // 2
    f = lambda ref: ref[...].astype(F32)
    out[:half] = block_of((f(low_a) + f(low_b) + f(low_c)).astype(BF16))
    out[half:] = block_of((f(high_a) + f(high_b) + f(high_c)).astype(BF16))


def combine_kernel(hidden, back, pair, out):
    rows = rows_of(back[...])
    both = dot(pair[...], rows, (0, 0))
    mixture = both[: out.shape[0]] + both[out.shape[0] :]
    out[...] = (hidden[...].astype(F32) + mixture).astype(BF16)


def sds(shape, dtype):
    return jax.ShapeDtypeStruct(shape, dtype)


def near(shape, dtype):
    return pltpu.VMEM(shape, dtype)


def nearby(*arrays):
    return tuple(pltpu.with_memory_space_constraint(a, pltpu.VMEM) for a in arrays)


def params(mib=24):
    return pltpu.CompilerParams(vmem_limit_bytes=mib << 20)


def distant(*arrays):
    return tuple(pltpu.with_memory_space_constraint(a, pltpu.HBM) for a in arrays)


VMEM = pl.BlockSpec(memory_space=pltpu.VMEM)


def cost(flops):
    return pl.CostEstimate(flops=flops, bytes_accessed=1 << 20, transcendentals=0)


def local(
    skip_stream,
    wide_probe_logits,
    narrow_probe_logits,
    wide_decay_logits,
    narrow_decay_logits,
    wide_floor_complement,
    narrow_floor_complement,
    payloads,
    result_switch_logits,
    spike_decays,
    channel_scale_vector,
    result_mapping_matrix,
    specialist_scale_vector,
    assignments,
    assignment_share,
    specialist_switch_matrix,
    specialist_raising_matrix,
    specialist_lowering_matrix,
):
    tokens, width = wide_probe_logits.shape
    rows, model = skip_stream.shape
    joint = payloads.shape[1]
    members = lax.axis_size(ZG)
    groups = lax.axis_size("zh")
    shards = lax.axis_size("tp")
    experts = lax.axis_size(SP)
    decay_args = (
        wide_decay_logits,
        narrow_decay_logits,
        wide_floor_complement,
        narrow_floor_complement,
        payloads,
        spike_decays.T,
    )

    summary = pl.pallas_call(
        summary_kernel,
        out_shape=near((members, PAY, width), BF16),
        compiler_params=params(),
        cost_estimate=cost(4 << 20),
    )(*distant(*decay_args))
    by_slice = lax.all_to_all(summary, ZG, 0, 0, tiled=True)
    slots = experts * CAP
    head_gain = channel_scale_vector.reshape(1, joint)
    chosen, share_pair, skip, norm_gain = pl.pallas_call(
        route_kernel,
        out_shape=[near((slots, rows), BF16), near((slots, 2 * rows), BF16)]
        + [near((rows, model), BF16), near((1, model), F32)],
        compiler_params=params(),
        cost_estimate=cost(1 << 20),
    )(
        *distant(
            assignments.T,
            assignment_share.T,
            skip_stream,
            specialist_scale_vector.reshape(1, model),
        )
    )
    inside, q_fwd, q_bwd, scale, projection = pl.pallas_call(
        local_kernel,
        in_specs=[VMEM] * 10 + [pl.BlockSpec(memory_space=pl.ANY)],
        out_shape=[
            near((tokens, joint), F32),
            near((tokens, 2 * width), BF16),
            near((tokens, 2 * width), BF16),
            near((tokens, joint), F32),
            near(result_mapping_matrix.shape, BF16),
        ],
        scratch_shapes=[pltpu.SemaphoreType.DMA],
        compiler_params=params(),
        cost_estimate=cost(64 << 20),
    )(
        *distant(
            wide_probe_logits,
            narrow_probe_logits,
            *decay_args,
            result_switch_logits,
            head_gain,
            result_mapping_matrix,
        )
    )
    before, decayed, total = pl.pallas_call(
        group_kernel,
        out_shape=[
            near((members, 2 * SLICE, width), F32),
            near((members, 2 * SLICE, width), F32),
            near((groups, PAY, width), BF16),
        ],
        compiler_params=params(),
        cost_estimate=cost(4 << 20),
    )(*nearby(by_slice))
    came = lax.all_to_all(total, "zh", 0, 0, tiled=True)
    carried = pl.pallas_call(
        carry_kernel,
        out_shape=near((members, 2 * SLICE, width), BF16),
        compiler_params=params(),
        cost_estimate=cost(4 << 20),
    )(*nearby(came, before, decayed))
    entering = lax.all_to_all(carried, ZG, 0, 0, tiled=True)
    mixed = pl.pallas_call(
        mix_kernel,
        out_shape=near((tokens, model), BF16),
        compiler_params=params(),
        cost_estimate=cost(256 << 20),
    )(*nearby(entering, inside, q_fwd, q_bwd, scale, projection))
    parts = lax.all_to_all(mixed.reshape(shards, rows, model), "tp", 0, 0, tiled=True)
    hidden, outgoing = pl.pallas_call(
        dispatch_kernel,
        out_shape=[near((rows, model), BF16), near((experts, CAP, model), BF16)],
        compiler_params=params(),
        cost_estimate=cost(16 << 20),
    )(*nearby(parts, skip, norm_gain, chosen))
    own = lax.all_to_all(outgoing, SP, 0, 0, tiled=True)

    up_ring = [(i, (i + 1) % shards) for i in range(shards)]
    down_ring = [(i, (i - 1) % shards) for i in range(shards)]

    def up(x):
        return lax.ppermute(x, "tp", up_ring)

    def down(x):
        return lax.ppermute(x, "tp", down_ring)

    half = slots // 2
    piece = near((half, model), BF16)

    def call(kernel, flops, *arrays, **rest):
        rest = {"out_shape": piece, **rest}
        return pl.pallas_call(
            kernel, compiler_params=params(), cost_estimate=cost(flops), **rest
        )(*arrays)

    weights = (
        specialist_switch_matrix[0],
        specialist_raising_matrix[0],
        specialist_lowering_matrix[0],
    )
    own_low, own_high = call(split_kernel, 1 << 20, *nearby(own), out_shape=[piece] * 2)
    left_low, right_high = up(own_low), down(own_high)
    left_high, right_low = up(own_high), down(own_low)
    sum_low, sum_high, *weights = call(
        own_kernel,
        2 << 30,
        *nearby(own_low, own_high),
        *distant(*weights),
        in_specs=[VMEM] * 2 + [pl.BlockSpec(memory_space=pl.ANY)] * 3,
        out_shape=[piece] * 2 + [near(w.shape, w.dtype) for w in weights],
        scratch_shapes=[pltpu.SemaphoreType.DMA((3,))],
    )

    def part(x, y):
        return call(piece_kernel, 2 << 30, *nearby(x, y, *weights), out_shape=[piece] * 2)

    def add(a, b):
        return call(add_kernel, 1 << 20, *nearby(a, b))

    far_low, far_high = up(left_low), down(right_high)
    for_left_low, for_right_high = part(left_low, right_high)
    got_high, got_low = up(for_right_high), down(for_left_low)
    for_left_high, for_right_low = part(left_high, right_low)
    for_far_low, for_far_high = part(far_low, far_high)
    add_low, add_high = up(for_far_low), down(for_far_high)
    last_low = up(add(for_right_low, add_low))
    last_high = down(add(for_left_high, add_high))
    summed = call(
        sum_kernel,
        1 << 20,
        *nearby(sum_low, last_low, got_low, sum_high, last_high, got_high),
        out_shape=near((experts, CAP, model), BF16),
    )
    back = lax.all_to_all(summed, SP, 0, 0, tiled=True)
    return pl.pallas_call(
        combine_kernel,
        out_shape=sds((rows, model), BF16),
        compiler_params=params(),
        cost_estimate=cost(16 << 20),
    )(*nearby(hidden, back, share_pair))


def solution(mesh):
    torus = Mesh(
        mesh.devices.reshape(mesh.shape["grp"], 4, 4, 2, mesh.shape["tp"]),
        GRP_SP_TP,
    )
    placed = (
        P(GRP_SP_TP, None),
        P(GRP_SP, "tp"),
        P(GRP_SP, "tp"),
        P(GRP_SP, "tp"),
        P(GRP_SP, "tp"),
        P(None, "tp"),
        P(None, "tp"),
        P(GRP_SP, "tp"),
        P(GRP_SP, "tp"),
        P(GRP_SP, "tp"),
        P("tp"),
        P("tp", None),
        P(),
        P(GRP_SP_TP, None),
        P(GRP_SP_TP, None),
        P(SP, None, "tp"),
        P(SP, None, "tp"),
        P(SP, "tp", None),
    )
    return jax.shard_map(
        local, mesh=torus, in_specs=placed, out_specs=P(GRP_SP_TP, None), check_vma=False
    )
```
